32 devices in a mesh: grp: 2 (over x), ep: 8 (over z, y), tp: 2 (over core).
Axes of the slice: x: 2, y: 2, z: 4, core: 2. Of those that a mesh axis runs over, the one named last changes fastest.
Arguments:
- tokens: bfloat16 [2304, 2048], P(('grp', 'ep')), parts along dimension 0, may hold values from -6 to 6
- norm_gain: bfloat16 [2048], replicated, may hold values from 0.099609375 to 1.8984375
- chosen_rows: int32 [16, 144], P('grp', 'ep'), parts along dimension 0, may hold values from 0 to 1151, as said below
- route_weights: float32 [16, 144], P('grp', 'ep'), parts along dimension 0, may hold values from 0.2 to 1
- gate_weight: bfloat16 [8, 2048, 1536], P('ep', None, 'tp'), may hold values from -0.125 to 0.125
- up_weight: bfloat16 [8, 2048, 1536], P('ep', None, 'tp'), may hold values from -0.125 to 0.125
- down_weight: bfloat16 [8, 1536, 2048], P('ep', 'tp'), may hold values from -0.15625 to 0.15625
Outputs:
- mixed: bfloat16 [2304, 2048], P(('grp', 'ep', 'tp')), parts along dimension 0
The draws below stay inside these ranges and needn't reach their ends.
There are 2 independent parts, one for each index of `grp`. The reference program is written for one: setup_inputs(seed, part) draws one part's arguments, and reference() takes and returns one part's arrays. A program takes and returns all parts, laid end to end along the dimension named above; an argument that names none is the same for every part. Nothing has to cross between parts.
Inputs may be any that keep to these rules, and one draw needn't show every extreme that they name: `chosen_rows`: the columns come in blocks of 18, one block for each index of ep's 144 tokens in order. In every row the first half of a block names distinct tokens of the first half of that block's tokens, and its second half distinct tokens of the second half.
All inputs are finite; a program needn't handle non-finite values.
Results may differ from the reference program's by a relative error of at most 0.01.
Values may be sent and summed in bfloat16 or wider, within the bound.
A program may use at most 128 MiB of HBM per device.

```python
import jax
import jax.numpy as jnp
from jax import lax

D = 2048
FF = 1536
TOK_DEV = 144
EXPERTS = 8
TOKENS = 1152
SLOTS = 18
CAP = 144
N_TP = 2


def draw_chosen_rows(key, part):
    sources = CAP // SLOTS
    half_rows = TOK_DEV // 2
    half_slots = SLOTS // 2
    scores = jax.random.randint(jax.random.fold_in(key, 11), (EXPERTS, sources, 2, half_rows), 0, 1048576)
    scores = scores * half_rows + jnp.arange(half_rows, dtype=jnp.int32)
    order = jnp.argsort(scores, axis=-1, stable=True)[..., :half_slots].astype(jnp.int32)
    source_ids = jnp.arange(sources, dtype=jnp.int32)[None, :, None, None] * TOK_DEV
    half_ids = jnp.arange(2, dtype=jnp.int32)[None, None, :, None] * half_rows
    rows = order + source_ids + half_ids
    return rows.reshape(EXPERTS, CAP).astype(jnp.int32)


def steps_of(rng, extent, shards, low, largest):
    loudness, own = 1.0, jax.random.fold_in(rng, 6)
    for dim, parts in shards:
        heights = jnp.exp(jax.random.uniform(jax.random.fold_in(own, dim), (parts,), jnp.float32, low / len(shards), largest / len(shards)))
        loudness = loudness * jnp.repeat(heights, extent[dim] // parts).reshape([-1 if axis == dim else 1 for axis in range(len(extent))])
    return loudness


def noise(rng, shape, deviation, most, shards=(), kind=jnp.bfloat16):
    result = deviation * jax.random.normal(rng, shape, jnp.float32)
    if shards:
        result = result * steps_of(rng, shape, shards, -0.22, 0.18)
    return jnp.clip(result, -most, most).astype(kind)


def setup_inputs(seed: int = 0, part: int = 0) -> dict:
    arg_keys = jax.random.split(jax.random.key(seed), 8)
    part_splits = jax.random.split(jax.random.fold_in(arg_keys[7], part), 8)
    return {
        "tokens": noise(part_splits[0], (TOKENS, D), 1.0, 6.0, ((0, 8),)),
        "norm_gain": jnp.clip(1.0 + 0.18 * jax.random.normal(arg_keys[1], (D,), jnp.float32), 0.099609375, 1.8984375).astype(jnp.bfloat16),
        "chosen_rows": draw_chosen_rows(jax.random.fold_in(jax.random.fold_in(arg_keys[7], part), 71), part),
        "route_weights": jnp.clip(0.2 + 0.8 * jax.random.uniform(part_splits[3], (EXPERTS, CAP), jnp.float32) ** steps_of(part_splits[3], (EXPERTS, CAP), ((1, 8),), -0.2, 0.2), 0.2, 1.0),
        "gate_weight": noise(arg_keys[4], (EXPERTS, D, FF), D ** -0.5, 0.125, ((0, 8), (2, 2))),
        "up_weight": noise(arg_keys[5], (EXPERTS, D, FF), D ** -0.5, 0.125, ((0, 8), (2, 2))),
        "down_weight": noise(arg_keys[6], (EXPERTS, FF, D), FF ** -0.5, 0.15625, ((0, 8), (1, 2))),
    }


def reference(tokens, norm_gain, chosen_rows, route_weights, gate_weight, up_weight, down_weight):
    values = tokens.astype(jnp.float32)
    scale = lax.rsqrt(lax.optimization_barrier(jnp.mean(values * values, axis=-1, keepdims=True)) + 1e-06)
    normed = (values * scale * norm_gain.astype(jnp.float32)).astype(jnp.bfloat16)
    half_ff = FF // N_TP

    def one_expert(total, inputs):
        expert_rows, expert_weights, w_gate, w_up, w_down = inputs
        expert_in = normed[expert_rows]
        gate_proj = jnp.dot(expert_in, w_gate, preferred_element_type=jnp.float32)
        up_proj = jnp.dot(expert_in, w_up, preferred_element_type=jnp.float32)
        hidden = (jax.nn.silu(gate_proj) * up_proj).astype(jnp.bfloat16)
        summed = jnp.zeros((expert_rows.shape[0], D), jnp.float32)
        for part_id in range(N_TP):
            partial_out = jnp.dot(hidden[:, part_id * half_ff:(part_id + 1) * half_ff], w_down[part_id * half_ff:(part_id + 1) * half_ff], preferred_element_type=jnp.float32).astype(jnp.bfloat16)
            partial_out = lax.optimization_barrier(partial_out)
            summed = summed + partial_out.astype(jnp.float32)
        expert_out = summed.astype(jnp.bfloat16)
        total = total.at[expert_rows].add(expert_weights[:, None] * expert_out.astype(jnp.float32))
        return (total, None)
    start_total = jnp.zeros((TOKENS, D), jnp.float32)
    total, unused = lax.scan(one_expert, start_total, (chosen_rows.astype(jnp.int32), route_weights, gate_weight, up_weight, down_weight))
    return total.astype(jnp.bfloat16)
```

```python
import functools

import jax
import jax.numpy as jnp
from jax import lax
from jax.experimental import pallas as pl
from jax.experimental.pallas import tpu as pltpu
from jax.sharding import PartitionSpec as P

MESH = pl.DeviceIdType.MESH
LANES = 128
PARTS = 2
CUTS = 1
TILE = 256
VMEM_BYTES = 67043328


phase = jax.named_scope


def loop(count, body):
    if count == 1:
        body(0)
    else:
        lax.fori_loop(0, count, lambda i, carry: (body(i), carry)[1], 0)


def each(low, high, body):
    lax.fori_loop(low, high, lambda i, carry: (body(i), carry)[1], 0)


def group_sizes(half):
    base = half // PARTS
    sizes = [base + (1 if i >= PARTS - half % PARTS else 0) for i in range(PARTS)]
    return [s for s in sizes if s]


def round_up(a, b):
    return (a + b - 1) // b * b


def kernel(
    n,
    tokens,
    gain_h,
    chosen_h,
    route_h,
    gate_w,
    up_w,
    down_w,
    mixed,
    tok,
    gain,
    chosen,
    route,
    wgu,
    wd,
    out_x,
    in_x,
    sib_x,
    flat,
    x_cols,
    hidden,
    p_send,
    p_recv,
    p_own,
    c_send,
    c_recv,
    g_rows,
    w_rows,
    spread,
    r_cols,
    load_sem,
    d_send,
    d_recv,
    f_send,
    f_recv,
    q_send,
    q_recv,
    b_send,
    b_recv,
    ready,
):
    tok_rows, width = tok.shape
    half_rows = tok_rows // 2
    experts, slots = chosen.shape
    half = slots // 2
    sizes = group_sizes(half)
    starts = [sum(sizes[:j]) for j in range(len(sizes))]
    chunks = range(len(sizes))
    side = n // 2
    quarter = n // 4
    bunch = min(side, 4)
    blocks = side // bunch
    pad = x_cols.shape[1] // 2
    pieces = width // LANES
    cols = width // CUTS
    f32, bf16 = jnp.float32, jnp.bfloat16
    me = lax.axis_index("ep")
    core = lax.axis_index("tp")
    sib = {"tp": 1 - core}
    upper = lax.div(me, side)
    spot = me - upper * side
    far_half = upper + core - 2 * upper * core
    base = far_half * side
    lower_far = core * (1 - upper)
    last_far = core * lax.div(me, 3 * quarter)

    barrier = pltpu.get_barrier_semaphore()

    def greet(semaphore, target):
        pl.semaphore_signal(semaphore, inc=1, device_id=target, device_id_type=MESH)

    greet(barrier, sib)
    near_first = 1 - core
    each(
        near_first,
        side * (1 - last_far),
        lambda i: greet(barrier, {"ep": base + lax.rem(spot * near_first + i, side)}),
    )
    load_tok = pltpu.make_async_copy(tokens, tok, load_sem.at[0])
    small = [
        pltpu.make_async_copy(src, dst, load_sem.at[i + 4])
        for i, (src, dst) in enumerate(((gain_h, gain), (chosen_h, chosen), (route_h, route)))
    ]
    small[1].start()
    load_tok.start()
    small[0].start()
    small[2].start()
    ff = wd.shape[0]
    loads = [
        pltpu.make_async_copy(src.at[0], dst, load_sem.at[i + 1])
        for i, (src, dst) in enumerate(
            (
                (gate_w, wgu.at[:, pl.ds(0, ff)]),
                (up_w, wgu.at[:, pl.ds(ff, ff)]),
                (down_w, wd),
            )
        )
    ]

    @pl.when(last_far == 1)
    def _():
        pl.semaphore_wait(barrier, 1 + side)
        each(0, side, lambda i: greet(ready, {"ep": i}))

    with phase("load"):
        small[1].wait()
    picked = (chosen[...] - me * tok_rows).astype(f32)
    mine_rows = jnp.where(far_half == 1, picked[side:], picked[:side])

    def hot_rows(j):
        size = sizes[j]
        rows = side * 2 * size
        row = lax.broadcasted_iota(jnp.int32, (rows, slots), 0)
        lane = lax.broadcasted_iota(jnp.int32, (rows, slots), 1)
        value = jnp.zeros((rows, slots), f32)
        want = jnp.zeros((rows, slots), jnp.int32)
        for k in range(side):
            for h in range(2):
                at = (2 * k + h) * size
                here = row >= at
                if h == 0:
                    value = jnp.where(here, mine_rows[k : k + 1, :], value)
                want = jnp.where(here, row + (h * half + starts[j] - at), want)
        index = jnp.sum(jnp.where(lane == want, value, 0.0), axis=-1, keepdims=True)
        token = lax.broadcasted_iota(jnp.int32, (rows, tok_rows), 1).astype(f32)
        return jnp.where(token == index, 1.0, 0.0)

    def block_rows(b, count):
        at = b * count
        return pl.ds(at if isinstance(b, int) else pl.multiple_of(at, count), count)

    def pack(value, ref, j, b):
        count = value.shape[0]
        for s in range(pieces):
            flat[pl.ds(s, count, stride=pieces), :] = value[:, s * LANES : (s + 1) * LANES]
        packed = flat[: count * pieces, :].reshape(count, pieces, LANES)
        ref[j, block_rows(b, count)] = packed.astype(bf16)

    def gather(j):
        count = bunch * 2 * sizes[j]
        with phase("hot"):
            g_rows[: blocks * count, :] = hot_rows(j)
        if j == 0:
            with phase("tok"):
                load_tok.wait()
                small[0].wait()
            for load in loads:
                load.start()

        def one(b):
            hot = g_rows[block_rows(b, count), :].astype(bf16)
            with phase("norm"):
                got = jnp.dot(hot, tok[...], preferred_element_type=f32)
                scale = lax.rsqrt(jnp.mean(got * got, axis=-1, keepdims=True) + 1e-06)
                got = got * scale * gain[...].astype(f32).reshape(1, width)
            with phase("pack"):
                pack(got, out_x, j, b)

        loop(blocks, one)

    def dispatch(j, low, high):
        count = 2 * sizes[j]

        def one(i):
            k = lax.rem(spot * near_first + i, side)
            pltpu.make_async_remote_copy(
                src_ref=out_x.at[j, pl.ds(k * count, count)],
                dst_ref=in_x.at[j, pl.ds(spot * count, count)],
                send_sem=d_send.at[j],
                recv_sem=d_recv.at[j],
                device_id={"ep": base + k},
                device_id_type=MESH,
            ).start()

        each(low, high, one)

    def keep_dispatch(j):
        count = 2 * sizes[j]

        @pl.when(core == 0)
        def _():
            for r in range(count):
                in_x[j, spot * count + r] = out_x[j, spot * count + r]

    def rows_copy(src, dst, j, rows, send_sem, recv_sem):
        return pltpu.make_async_remote_copy(
            src_ref=src.at[j, pl.ds(0, rows)],
            dst_ref=dst.at[j, pl.ds(0, rows)],
            send_sem=send_sem.at[j],
            recv_sem=recv_sem.at[j],
            device_id=sib,
            device_id_type=MESH,
        )

    def by_core(rows_even, rows_odd, wait):
        @pl.when(core == 0)
        def _():
            wait(rows_even)

        @pl.when(core == 1)
        def _():
            wait(rows_odd)

    def dispatched(j, sent):
        count = 2 * sizes[j]

        def wait(rows):
            copy = rows_copy(out_x, in_x, j, rows, d_send, d_recv)
            copy.wait_send() if sent else copy.wait_recv()

        by_core((side - 1) * count, side * count, wait)

    def returned(j, sent):
        def wait(rows):
            copy = rows_copy(c_recv, c_recv, j, rows, b_send, b_recv)
            copy.wait_send() if sent else copy.wait_recv()

        by_core((n - 1) * sizes[j], n * sizes[j], wait)

    def forward(j):
        return rows_copy(in_x, sib_x, j, side * 2 * sizes[j], f_send, f_recv)

    def swap(j, k):
        return pltpu.make_async_remote_copy(
            src_ref=p_send.at[j, k],
            dst_ref=p_recv.at[j, k],
            send_sem=q_send.at[CUTS * j + k],
            recv_sem=q_recv.at[CUTS * j + k],
            device_id=sib,
            device_id_type=MESH,
        )

    def give_back(j):
        size = sizes[j]

        first = near_first * spot + core * (1 - upper) * quarter

        def one(i):
            k = lax.rem(first + i, side)
            for h in range(2):
                pltpu.make_async_remote_copy(
                    src_ref=c_send.at[j, pl.ds((2 * k + h) * size, size)],
                    dst_ref=c_recv.at[j, pl.ds(me * size, size)],
                    send_sem=b_send.at[j],
                    recv_sem=b_recv.at[j],
                    device_id={"ep": base + k, "tp": h},
                    device_id_type=MESH,
                ).start()

        each(near_first, side, one)

        @pl.when(core == 0)
        def _():
            pltpu.make_async_remote_copy(
                src_ref=c_send.at[j, pl.ds((2 * spot + 1) * size, size)],
                dst_ref=c_recv.at[j, pl.ds(me * size, size)],
                send_sem=b_send.at[j],
                recv_sem=b_recv.at[j],
                device_id=sib,
                device_id_type=MESH,
            ).start()
            for r in range(size):
                c_recv[j, me * size + r] = c_send[j, 2 * spot * size + r]

    def arrive(j):
        with phase(f"arrive{j}"):
            dispatched(j, False)
            forward(j).start()

    def to_cols(ref, j, at):
        count = bunch * 2 * sizes[j]

        def one(b):
            got = ref[j, block_rows(b, count)].astype(f32)
            flat[pl.ds(0, count * pieces), :] = got.reshape(count * pieces, LANES)
            for s in range(pieces):
                x_cols[b, at : at + count, s * LANES : (s + 1) * LANES] = flat[
                    pl.ds(s, count, stride=pieces), :
                ].astype(bf16)

        loop(blocks, one)

    def project(j):
        def one(b):
            for c in range(0, ff, TILE):
                gate = jnp.dot(x_cols[b], wgu[:, c : c + TILE], preferred_element_type=f32)
                up = jnp.dot(x_cols[b], wgu[:, ff + c : ff + c + TILE], preferred_element_type=f32)
                hidden[b, :, c : c + TILE] = (gate / (1.0 + jnp.exp(-gate)) * up).astype(bf16)

        loop(blocks, one)

    def down(j):
        count = bunch * 2 * sizes[j]
        for k in range(CUTS):
            part = slice(k * cols, (k + 1) * cols)

            def one(b):
                got = jnp.dot(hidden[b], wd[:, part], preferred_element_type=f32)
                p_send[j, k, b, :count] = got[pad : pad + count].astype(bf16)
                p_own[j, k, b, :count] = got[:count].astype(bf16)

            loop(blocks, one)
            swap(j, k).start()

    def combine(j):
        count = bunch * 2 * sizes[j]

        def one(b):
            both = [
                p_own[j, k, b, :count].astype(f32) + p_recv[j, k, b, :count].astype(f32)
                for k in range(CUTS)
            ]
            pack(jnp.concatenate(both, axis=1), c_send, j, b)

        loop(blocks, one)

    def finish(j):
        with phase(f"swap{j}"):
            for k in range(CUTS):
                swap(j, k).wait_recv()
        with phase(f"combine{j}"):
            combine(j)
            give_back(j)

    for j in chunks:
        with phase(f"gather{j}"):
            gather(j)
        if j == 0:

            with phase("enter"):

                @pl.when(last_far == 0)
                def _():
                    entered = side * (1 - lower_far) + (1 + quarter) * lower_far + core * upper
                    pl.semaphore_wait(barrier, entered)

        dispatch(j, near_first, side - quarter * lower_far)
        keep_dispatch(j)

    with phase("ready"):

        @pl.when(lower_far == 1)
        def _():
            pl.semaphore_wait(ready, quarter)
            for j in chunks:
                dispatch(j, quarter, side)

    small[2].wait()
    mine = (picked - core * half_rows).T
    weight = route[...].T
    lane = lax.broadcasted_iota(jnp.int32, (half, half_rows), 1).astype(f32)
    for e in range(experts):
        pair = [mine[h * half : (h + 1) * half, e : e + 1] for h in range(2)]
        row = jnp.where(core == 0, pair[0], pair[1])
        pair = [weight[h * half : (h + 1) * half, e : e + 1] for h in range(2)]
        share = jnp.where(core == 0, pair[0], pair[1])
        here = jnp.where(lane == row, share, 0.0)
        for j, size in enumerate(sizes):
            at = experts * starts[j] + e * size
            w_rows[at : at + size, :] = here[starts[j] : starts[j] + size]
    turned = w_rows[...].T
    high = turned.astype(bf16)
    spread[:half_rows, :] = high.astype(f32)
    spread[half_rows:, :] = turned - high.astype(f32)
    x_cols[...] = jnp.zeros(x_cols.shape, bf16)

    arrive(0)
    for load in loads[:2]:
        load.wait()
    for j in chunks:
        with phase(f"cols{j}"):
            to_cols(in_x, j, 0)
        with phase(f"forward{j}"):
            forward(j).wait_recv()
        if j + 1 < len(sizes):

            @pl.when(core == 0)
            def _():
                arrive(j + 1)

        with phase(f"sib{j}"):
            to_cols(sib_x, j, pad)
        with phase(f"project{j}"):
            project(j)
        if j > 0:
            finish(j - 1)
        if j + 1 < len(sizes):

            @pl.when(core == 1)
            def _():
                arrive(j + 1)

        if j == 0:
            loads[2].wait()
        with phase(f"down{j}"):
            down(j)
    finish(len(sizes) - 1)

    for j in chunks:
        with phase(f"returned{j}"):
            returned(j, False)
        block = 8 * sizes[j]

        def unpack(b):
            got = c_recv[j, block_rows(b, block)].astype(f32)
            flat[: block * pieces, :] = got.reshape(block * pieces, LANES)
            at = experts * starts[j] + b * block
            at = at if isinstance(b, int) else pl.multiple_of(at, 8)
            for s in range(pieces):
                r_cols[pl.ds(at, block), s * LANES : (s + 1) * LANES] = flat[
                    pl.ds(s, block, stride=pieces), :
                ]

        loop(experts // 8, unpack)
    for k in range(CUTS):
        part = slice(k * cols, (k + 1) * cols)
        res = r_cols[:, part].astype(bf16)
        total = jnp.dot(spread[...].astype(bf16), res, preferred_element_type=f32)
        mixed[:, part] = (total[:half_rows] + total[half_rows:]).astype(bf16)

    for j in chunks:
        dispatched(j, True)
        forward(j).wait_send()
        for k in range(CUTS):
            swap(j, k).wait_send()
        returned(j, True)


def local(n, tokens, norm_gain, chosen_rows, route_weights, gate_weight, up_weight, down_weight):
    tok_rows, width = tokens.shape
    half_rows = tok_rows // 2
    experts, slots = chosen_rows.shape
    half = slots // 2
    rows = experts * half
    sizes = group_sizes(half)
    parts = len(sizes)
    top = max(sizes)
    side = n // 2
    bunch = min(side, 4)
    blocks = side // bunch
    block = bunch * 2 * top
    pad = round_up(block, 16)
    pieces = width // LANES
    ff = gate_weight.shape[2]
    bf16, f32 = jnp.bfloat16, jnp.float32
    packed = pltpu.VMEM((parts, n * top, pieces, LANES), bf16)
    partial = pltpu.VMEM((parts, CUTS, blocks, block, width // CUTS), bf16)
    vmem = pl.BlockSpec(memory_space=pltpu.VMEM)
    hbm = pl.BlockSpec(memory_space=pltpu.HBM)
    scratch = [
        pltpu.VMEM((tok_rows, width), bf16),
        pltpu.VMEM(norm_gain.shape, norm_gain.dtype),
        pltpu.VMEM(chosen_rows.shape, chosen_rows.dtype),
        pltpu.VMEM(route_weights.shape, route_weights.dtype),
        pltpu.VMEM((width, 2 * ff), bf16),
        pltpu.VMEM(down_weight.shape[1:], bf16),
        packed,
        packed,
        packed,
        pltpu.VMEM((max(block, 8 * top) * pieces, LANES), f32),
        pltpu.VMEM((blocks, 2 * pad, width), bf16),
        pltpu.VMEM((blocks, 2 * pad, ff), bf16),
        partial,
        partial,
        partial,
        packed,
        packed,
        pltpu.VMEM((n * top, tok_rows), f32),
        pltpu.VMEM((rows, half_rows), f32),
        pltpu.VMEM((tok_rows, rows), f32),
        pltpu.VMEM((rows, width), f32),
    ]
    limit = VMEM_BYTES - half_rows * width * 2
    return pl.pallas_call(
        functools.partial(kernel, n),
        out_shape=pltpu.VMEM((half_rows, width), bf16),
        in_specs=[hbm] * 7,
        out_specs=vmem,
        scratch_shapes=scratch
        + [pltpu.SemaphoreType.DMA((7,))]
        + [pltpu.SemaphoreType.DMA((CUTS * parts,))] * 8
        + [pltpu.SemaphoreType.REGULAR],
        compiler_params=pltpu.CompilerParams(
            collective_id=0, has_side_effects=True, vmem_limit_bytes=limit
        ),
    )(
        tokens,
        norm_gain,
        chosen_rows,
        route_weights,
        gate_weight,
        up_weight,
        down_weight,
    )


def solution(mesh):
    return jax.shard_map(
        functools.partial(local, mesh.shape["ep"]),
        mesh=mesh,
        in_specs=(
            P(("grp", "ep"), None),
            P(),
            P("grp", "ep"),
            P("grp", "ep"),
            P("ep", None, "tp"),
            P("ep", None, "tp"),
            P("ep", "tp", None),
        ),
        out_specs=P(("grp", "ep", "tp"), None),
        check_vma=False,
    )
```

```python
import functools

import jax
import jax.numpy as jnp
from jax import lax
from jax.experimental import pallas as pl
from jax.experimental.pallas import tpu as pltpu
from jax.sharding import PartitionSpec as P

MESH = pl.DeviceIdType.MESH
LANES = 128
PARTS = 2
CUTS = 1
TILE = 256
VMEM_BYTES = 67043328


phase = jax.named_scope


def loop(count, body):
    if count == 1:
        body(0)
    else:
        lax.fori_loop(0, count, lambda i, carry: (body(i), carry)[1], 0)


def each(low, high, body):
    lax.fori_loop(low, high, lambda i, carry: (body(i), carry)[1], 0)


def group_sizes(half):
    base = half // PARTS
    sizes = [base + (1 if i >= PARTS - half % PARTS else 0) for i in range(PARTS)]
    return [s for s in sizes if s]


def round_up(a, b):
    return (a + b - 1) // b * b


def kernel(
    n,
    tokens,
    gain_h,
    chosen_h,
    route_h,
    gate_w,
    up_w,
    down_w,
    mixed,
    tok,
    gain,
    chosen,
    route,
    wgu,
    wd,
    out_x,
    in_x,
    sib_x,
    relay_x,
    flat,
    x_cols,
    hidden,
    p_send,
    p_recv,
    p_own,
    c_send,
    c_recv,
    g_rows,
    w_rows,
    spread,
    r_cols,
    d_send,
    d_recv,
    f_send,
    f_recv,
    q_send,
    q_recv,
    b_send,
    b_recv,
    r_send,
    r_recv,
    h_send,
    ready,
):
    tok_rows, width = tok.shape
    half_rows = tok_rows // 2
    experts, slots = chosen.shape
    half = slots // 2
    sizes = group_sizes(half)
    starts = [sum(sizes[:j]) for j in range(len(sizes))]
    chunks = range(len(sizes))
    side = n // 2
    quarter = n // 4
    bunch = min(side, 4)
    blocks = side // bunch
    pad = x_cols.shape[1] // 2
    pieces = width // LANES
    cols = width // CUTS
    f32, bf16 = jnp.float32, jnp.bfloat16
    me = lax.axis_index("ep")
    core = lax.axis_index("tp")
    sib = {"tp": 1 - core}
    upper = lax.div(me, side)
    spot = me - upper * side
    far_half = upper + core - 2 * upper * core
    base = far_half * side
    place = lax.div(me, quarter)
    role = [core * jnp.where(place == i, 1, 0) for i in range(4)]

    barrier = pltpu.get_barrier_semaphore()

    def greet(semaphore, target):
        pl.semaphore_signal(semaphore, inc=1, device_id=target, device_id_type=MESH)

    greet(barrier, sib)
    near_first = 1 - core
    each(
        near_first + quarter * role[2],
        side * (1 - role[3]),
        lambda i: greet(barrier, {"ep": base + lax.rem(spot * near_first + i, side)}),
    )

    @pl.when(role[1] == 1)
    def _():
        greet(barrier, {"ep": me - quarter})

    load_tok = pltpu.make_async_copy(tokens, tok, h_send.at[0])
    small = [
        pltpu.make_async_copy(src, dst, sem)
        for src, dst, sem in (
            (gain_h, gain, h_send.at[1]),
            (chosen_h, chosen, b_send.at[1]),
            (route_h, route, f_send.at[0]),
        )
    ]
    small[1].start()
    load_tok.start()
    small[0].start()
    small[2].start()
    ff = wd.shape[0]
    loads = [
        pltpu.make_async_copy(src.at[0], dst, sem)
        for src, dst, sem in (
            (gate_w, wgu.at[:, pl.ds(0, ff)], q_send.at[0]),
            (up_w, wgu.at[:, pl.ds(ff, ff)], q_send.at[1]),
            (down_w, wd, b_send.at[0]),
        )
    ]

    @pl.when(role[3] == 1)
    def _():
        pl.semaphore_wait(barrier, 1 + side)
        each(quarter, side, lambda i: greet(ready, {"ep": i}))

    with phase("load"):
        small[1].wait()
    picked = (chosen[...] - me * tok_rows).astype(f32)
    mine_rows = jnp.where(far_half == 1, picked[side:], picked[:side])

    def hot_rows(j):
        size = sizes[j]
        rows = side * 2 * size
        row = lax.broadcasted_iota(jnp.int32, (rows, slots), 0)
        lane = lax.broadcasted_iota(jnp.int32, (rows, slots), 1)
        value = jnp.zeros((rows, slots), f32)
        want = jnp.zeros((rows, slots), jnp.int32)
        for k in range(side):
            for h in range(2):
                at = (2 * k + h) * size
                here = row >= at
                if h == 0:
                    value = jnp.where(here, mine_rows[k : k + 1, :], value)
                want = jnp.where(here, row + (h * half + starts[j] - at), want)
        index = jnp.sum(jnp.where(lane == want, value, 0.0), axis=-1, keepdims=True)
        token = lax.broadcasted_iota(jnp.int32, (rows, tok_rows), 1).astype(f32)
        return jnp.where(token == index, 1.0, 0.0)

    def block_rows(b, count):
        at = b * count
        return pl.ds(at if isinstance(b, int) else pl.multiple_of(at, count), count)

    def pack(value, ref, j, b):
        count = value.shape[0]
        for s in range(pieces):
            flat[pl.ds(s, count, stride=pieces), :] = value[:, s * LANES : (s + 1) * LANES]
        packed = flat[: count * pieces, :].reshape(count, pieces, LANES)
        ref[j, block_rows(b, count)] = packed.astype(bf16)

    def gather(j):
        count = bunch * 2 * sizes[j]
        with phase("hot"):
            g_rows[: blocks * count, :] = hot_rows(j)
        if j == 0:
            with phase("tok"):
                load_tok.wait()
                small[0].wait()
            for load in loads:
                load.start()

        def one(b):
            hot = g_rows[block_rows(b, count), :].astype(bf16)
            with phase("norm"):
                got = jnp.dot(hot, tok[...], preferred_element_type=f32)
                scale = lax.rsqrt(jnp.mean(got * got, axis=-1, keepdims=True) + 1e-06)
                got = got * scale * gain[...].astype(f32).reshape(1, width)
            with phase("pack"):
                pack(got, out_x, j, b)

        loop(blocks, one)

    def dispatch(j, low, high):
        count = 2 * sizes[j]

        def one(i):
            k = lax.rem(spot * near_first + i, side)
            pltpu.make_async_remote_copy(
                src_ref=out_x.at[j, pl.ds(k * count, count)],
                dst_ref=in_x.at[j, pl.ds(spot * count, count)],
                send_sem=d_send.at[j],
                recv_sem=d_recv.at[j],
                device_id={"ep": base + k},
                device_id_type=MESH,
            ).start()

        each(low, high, one)

    def part_rows(j, p):
        count = quarter * 2 * sizes[j]
        return pl.ds(p * count, count)

    def relay(j, p):
        return pltpu.make_async_remote_copy(
            src_ref=out_x.at[j, part_rows(j, p)],
            dst_ref=relay_x.at[j, part_rows(j, p)],
            send_sem=r_send.at[2 * j + p],
            recv_sem=r_recv.at[2 * j + p],
            device_id={"ep": me + quarter},
            device_id_type=MESH,
        )

    def pass_on(j, p):
        count = 2 * sizes[j]
        relay(j, p).wait_recv()

        def one(k):
            pltpu.make_async_remote_copy(
                src_ref=relay_x.at[j, pl.ds(k * count, count)],
                dst_ref=in_x.at[j, pl.ds((spot - quarter) * count, count)],
                send_sem=h_send.at[j],
                recv_sem=d_recv.at[j],
                device_id={"ep": base + k},
                device_id_type=MESH,
            ).start()

        each(p * quarter, (p + 1) * quarter, one)

    def keep_dispatch(j):
        count = 2 * sizes[j]

        @pl.when(core == 0)
        def _():
            for r in range(count):
                in_x[j, spot * count + r] = out_x[j, spot * count + r]

    def rows_copy(src, dst, j, rows, send_sem, recv_sem):
        return pltpu.make_async_remote_copy(
            src_ref=src.at[j, pl.ds(0, rows)],
            dst_ref=dst.at[j, pl.ds(0, rows)],
            send_sem=send_sem.at[j],
            recv_sem=recv_sem.at[j],
            device_id=sib,
            device_id_type=MESH,
        )

    def by_core(rows_even, rows_odd, wait):
        @pl.when(core == 0)
        def _():
            wait(rows_even)

        @pl.when(core == 1)
        def _():
            wait(rows_odd)

    def dispatched(j):
        count = 2 * sizes[j]
        by_core(
            (side - 1) * count,
            side * count,
            lambda rows: rows_copy(out_x, in_x, j, rows, d_send, d_recv).wait_recv(),
        )

    def dispatch_left(j):
        count = 2 * sizes[j]

        @pl.when(core == 0)
        def _():
            rows_copy(out_x, in_x, j, (side - 1) * count, d_send, d_recv).wait_send()

        @pl.when(core - role[0] == 1)
        def _():
            rows_copy(out_x, in_x, j, side * count, d_send, d_recv).wait_send()

        @pl.when(role[0] == 1)
        def _():
            for p in range(2):
                relay(j, p).wait_send()

        @pl.when(role[1] == 1)
        def _():
            rows_copy(relay_x, in_x, j, side * count, h_send, d_recv).wait_send()

    def returned(j, sent):
        def wait(rows):
            copy = rows_copy(c_recv, c_recv, j, rows, b_send, b_recv)
            copy.wait_send() if sent else copy.wait_recv()

        by_core((n - 1) * sizes[j], n * sizes[j], wait)

    def forward(j):
        return rows_copy(in_x, sib_x, j, side * 2 * sizes[j], f_send, f_recv)

    def swap(j, k):
        return pltpu.make_async_remote_copy(
            src_ref=p_send.at[j, k],
            dst_ref=p_recv.at[j, k],
            send_sem=q_send.at[CUTS * j + k],
            recv_sem=q_recv.at[CUTS * j + k],
            device_id=sib,
            device_id_type=MESH,
        )

    def give_back(j):
        size = sizes[j]

        first = near_first * spot + (role[0] + role[1]) * quarter

        def one(i):
            k = lax.rem(first + i, side)
            for h in range(2):
                pltpu.make_async_remote_copy(
                    src_ref=c_send.at[j, pl.ds((2 * k + h) * size, size)],
                    dst_ref=c_recv.at[j, pl.ds(me * size, size)],
                    send_sem=b_send.at[j],
                    recv_sem=b_recv.at[j],
                    device_id={"ep": base + k, "tp": h},
                    device_id_type=MESH,
                ).start()

        each(near_first, side, one)

        @pl.when(core == 0)
        def _():
            pltpu.make_async_remote_copy(
                src_ref=c_send.at[j, pl.ds((2 * spot + 1) * size, size)],
                dst_ref=c_recv.at[j, pl.ds(me * size, size)],
                send_sem=b_send.at[j],
                recv_sem=b_recv.at[j],
                device_id=sib,
                device_id_type=MESH,
            ).start()
            for r in range(size):
                c_recv[j, me * size + r] = c_send[j, 2 * spot * size + r]

    def arrive(j):
        with phase(f"arrive{j}"):
            dispatched(j)
            forward(j).start()

    def to_cols(ref, j, at):
        count = bunch * 2 * sizes[j]

        def one(b):
            got = ref[j, block_rows(b, count)].astype(f32)
            flat[pl.ds(0, count * pieces), :] = got.reshape(count * pieces, LANES)
            for s in range(pieces):
                x_cols[b, at : at + count, s * LANES : (s + 1) * LANES] = flat[
                    pl.ds(s, count, stride=pieces), :
                ].astype(bf16)

        loop(blocks, one)

    def project(j):
        def one(b):
            for c in range(0, ff, TILE):
                gate = jnp.dot(x_cols[b], wgu[:, c : c + TILE], preferred_element_type=f32)
                up = jnp.dot(x_cols[b], wgu[:, ff + c : ff + c + TILE], preferred_element_type=f32)
                hidden[b, :, c : c + TILE] = (gate / (1.0 + jnp.exp(-gate)) * up).astype(bf16)

        loop(blocks, one)

    def down(j):
        count = bunch * 2 * sizes[j]
        for k in range(CUTS):
            part = slice(k * cols, (k + 1) * cols)

            def one(b):
                got = jnp.dot(hidden[b], wd[:, part], preferred_element_type=f32)
                p_send[j, k, b, :count] = got[pad : pad + count].astype(bf16)
                p_own[j, k, b, :count] = got[:count].astype(bf16)

            loop(blocks, one)
            swap(j, k).start()

    def combine(j):
        count = bunch * 2 * sizes[j]

        def one(b):
            both = [
                p_own[j, k, b, :count].astype(f32) + p_recv[j, k, b, :count].astype(f32)
                for k in range(CUTS)
            ]
            pack(jnp.concatenate(both, axis=1), c_send, j, b)

        loop(blocks, one)

    def finish(j):
        with phase(f"swap{j}"):
            for k in range(CUTS):
                swap(j, k).wait_recv()
        with phase(f"combine{j}"):
            combine(j)
            give_back(j)

    for j in chunks:
        with phase(f"gather{j}"):
            gather(j)
        if j == 0:

            with phase("enter"):

                @pl.when(role[3] == 0)
                def _():
                    entered = side * (1 - core) + 2 * role[0]
                    entered = entered + (1 + quarter) * role[1] + (1 + side) * role[2]
                    pl.semaphore_wait(barrier, entered)

        dispatch(j, near_first, side * (1 - role[0]) - quarter * role[1])
        keep_dispatch(j)

        @pl.when(role[0] == 1)
        def _():
            relay(j, 1).start()
            relay(j, 0).start()

    small[2].wait()
    mine = (picked - core * half_rows).T
    weight = route[...].T
    lane = lax.broadcasted_iota(jnp.int32, (half, half_rows), 1).astype(f32)
    for e in range(experts):
        pair = [mine[h * half : (h + 1) * half, e : e + 1] for h in range(2)]
        row = jnp.where(core == 0, pair[0], pair[1])
        pair = [weight[h * half : (h + 1) * half, e : e + 1] for h in range(2)]
        share = jnp.where(core == 0, pair[0], pair[1])
        here = jnp.where(lane == row, share, 0.0)
        for j, size in enumerate(sizes):
            at = experts * starts[j] + e * size
            w_rows[at : at + size, :] = here[starts[j] : starts[j] + size]
    turned = w_rows[...].T
    high = turned.astype(bf16)
    spread[:half_rows, :] = high.astype(f32)
    spread[half_rows:, :] = turned - high.astype(f32)
    x_cols[...] = jnp.zeros(x_cols.shape, bf16)

    with phase("ready"):

        @pl.when(role[1] == 1)
        def _():
            pl.semaphore_wait(ready, quarter)
            dispatch(0, quarter, side)
            pass_on(0, 1)
            pass_on(0, 0)
            for j in chunks[1:]:
                dispatch(j, quarter, side)

    arrive(0)
    with phase("pass"):

        @pl.when(role[1] == 1)
        def _():
            for j in chunks[1:]:
                pass_on(j, 1)
                pass_on(j, 0)

    for load in loads[:2]:
        load.wait()
    last = len(sizes) - 1
    late = upper * (1 - core)
    soon = upper * core
    for j in chunks:
        with phase(f"cols{j}"):
            to_cols(in_x, j, 0)
        if j > 0:

            @pl.when(late == 0)
            def _():
                finish(j - 1)

        with phase(f"forward{j}"):
            forward(j).wait_recv()
        with phase(f"sib{j}"):
            to_cols(sib_x, j, pad)
        with phase(f"project{j}"):
            project(j)
        if j < last:

            @pl.when(soon == 1)
            def _():
                arrive(j + 1)

        if j == 0:
            loads[2].wait()
        with phase(f"down{j}"):
            down(j)
        if j < last:

            @pl.when(soon == 0)
            def _():
                arrive(j + 1)

        if j > 0:

            @pl.when(late == 1)
            def _():
                finish(j - 1)

    with phase("left"):
        for j in chunks:
            dispatch_left(j)
            forward(j).wait_send()
    finish(last)
    with phase("left"):
        for j in chunks:
            for k in range(CUTS):
                swap(j, k).wait_send()
        for j in chunks[:last]:
            returned(j, True)

    for j in chunks:
        if j == last:
            returned(j, True)
        with phase(f"returned{j}"):
            returned(j, False)
        block = 8 * sizes[j]

        def unpack(b):
            got = c_recv[j, block_rows(b, block)].astype(f32)
            flat[: block * pieces, :] = got.reshape(block * pieces, LANES)
            at = experts * starts[j] + b * block
            at = at if isinstance(b, int) else pl.multiple_of(at, 8)
            for s in range(pieces):
                r_cols[pl.ds(at, block), s * LANES : (s + 1) * LANES] = flat[
                    pl.ds(s, block, stride=pieces), :
                ]

        loop(experts // 8, unpack)
    for k in range(CUTS):
        part = slice(k * cols, (k + 1) * cols)
        res = r_cols[:, part].astype(bf16)
        total = jnp.dot(spread[...].astype(bf16), res, preferred_element_type=f32)
        mixed[:, part] = (total[:half_rows] + total[half_rows:]).astype(bf16)


def local(n, tokens, norm_gain, chosen_rows, route_weights, gate_weight, up_weight, down_weight):
    tok_rows, width = tokens.shape
    half_rows = tok_rows // 2
    experts, slots = chosen_rows.shape
    half = slots // 2
    rows = experts * half
    sizes = group_sizes(half)
    parts = len(sizes)
    top = max(sizes)
    side = n // 2
    bunch = min(side, 4)
    blocks = side // bunch
    block = bunch * 2 * top
    pad = round_up(block, 16)
    pieces = width // LANES
    ff = gate_weight.shape[2]
    bf16, f32 = jnp.bfloat16, jnp.float32
    packed = pltpu.VMEM((parts, n * top, pieces, LANES), bf16)
    partial = pltpu.VMEM((parts, CUTS, blocks, block, width // CUTS), bf16)
    vmem = pl.BlockSpec(memory_space=pltpu.VMEM)
    hbm = pl.BlockSpec(memory_space=pltpu.HBM)
    scratch = [
        pltpu.VMEM((tok_rows, width), bf16),
        pltpu.VMEM(norm_gain.shape, norm_gain.dtype),
        pltpu.VMEM(chosen_rows.shape, chosen_rows.dtype),
        pltpu.VMEM(route_weights.shape, route_weights.dtype),
        pltpu.VMEM((width, 2 * ff), bf16),
        pltpu.VMEM(down_weight.shape[1:], bf16),
        packed,
        packed,
        packed,
        packed,
        pltpu.VMEM((max(block, 8 * top) * pieces, LANES), f32),
        pltpu.VMEM((blocks, 2 * pad, width), bf16),
        pltpu.VMEM((blocks, 2 * pad, ff), bf16),
        partial,
        partial,
        partial,
        packed,
        packed,
        pltpu.VMEM((n * top, tok_rows), f32),
        pltpu.VMEM((rows, half_rows), f32),
        pltpu.VMEM((tok_rows, rows), f32),
        pltpu.VMEM((rows, width), f32),
    ]
    limit = VMEM_BYTES - half_rows * width * 2
    return pl.pallas_call(
        functools.partial(kernel, n),
        out_shape=pltpu.VMEM((half_rows, width), bf16),
        in_specs=[hbm] * 7,
        out_specs=vmem,
        scratch_shapes=scratch
        + [pltpu.SemaphoreType.DMA((parts,))] * 8
        + [pltpu.SemaphoreType.DMA((2 * parts,))] * 2
        + [pltpu.SemaphoreType.DMA((parts,))]
        + [pltpu.SemaphoreType.REGULAR],
        compiler_params=pltpu.CompilerParams(
            collective_id=0, has_side_effects=True, vmem_limit_bytes=limit
        ),
    )(
        tokens,
        norm_gain,
        chosen_rows,
        route_weights,
        gate_weight,
        up_weight,
        down_weight,
    )


def solution(mesh):
    return jax.shard_map(
        functools.partial(local, mesh.shape["ep"]),
        mesh=mesh,
        in_specs=(
            P(("grp", "ep"), None),
            P(),
            P("grp", "ep"),
            P("grp", "ep"),
            P("ep", None, "tp"),
            P("ep", None, "tp"),
            P("ep", "tp", None),
        ),
        out_specs=P(("grp", "ep", "tp"), None),
        check_vma=False,
    )
```

```python
import functools

import jax
import jax.numpy as jnp
from jax import lax
from jax.experimental import pallas as pl
from jax.experimental.pallas import tpu as pltpu
from jax.sharding import PartitionSpec as P

MESH = pl.DeviceIdType.MESH
LANES = 128
PARTS = 2
TILE = 256
VMEM_BYTES = 67043328


phase = jax.named_scope


def loop(count, body):
    if count == 1:
        body(0)
    else:
        lax.fori_loop(0, count, lambda i, carry: (body(i), carry)[1], 0)


def each(low, high, body):
    lax.fori_loop(low, high, lambda i, carry: (body(i), carry)[1], 0)


def group_sizes(half):
    base = half // PARTS
    sizes = [base + (1 if i >= PARTS - half % PARTS else 0) for i in range(PARTS)]
    return [s for s in sizes if s]


def round_up(a, b):
    return (a + b - 1) // b * b


def kernel(
    n,
    tokens,
    gain_h,
    chosen_h,
    route_h,
    gate_w,
    up_w,
    down_w,
    mixed,
    tok,
    gain,
    chosen,
    route,
    wgu,
    wd,
    out_x,
    in_x,
    relay_x,
    flat,
    x_cols,
    sums,
    p_recv,
    c_send,
    c_recv,
    g_rows,
    w_rows,
    spread,
    r_cols,
    d_send,
    d_recv,
    f_send,
    f_recv,
    q_send,
    q_recv,
    b_send,
    b_recv,
    r_send,
    r_recv,
    h_send,
    ready,
):
    tok_rows, width = tok.shape
    half_rows = tok_rows // 2
    experts, slots = chosen.shape
    half = slots // 2
    sizes = group_sizes(half)
    starts = [sum(sizes[:j]) for j in range(len(sizes))]
    chunks = range(len(sizes))
    side = n // 2
    quarter = n // 4
    bunch = min(side, 4)
    blocks = side // bunch
    pad = round_up(bunch * 2 * max(sizes), 16)
    first_pad = round_up(bunch * 2 * sizes[0], 16)
    pieces = width // LANES
    cols = width // 2
    f32, bf16 = jnp.float32, jnp.bfloat16
    me = lax.axis_index("ep")
    core = lax.axis_index("tp")
    sib = {"tp": 1 - core}
    upper = lax.div(me, side)
    spot = me - upper * side
    far_half = upper + core - 2 * upper * core
    base = far_half * side
    place = lax.div(me, quarter)
    role = [core * jnp.where(place == i, 1, 0) for i in range(4)]

    barrier = pltpu.get_barrier_semaphore()

    def greet(semaphore, target):
        pl.semaphore_signal(semaphore, inc=1, device_id=target, device_id_type=MESH)

    greet(barrier, sib)
    even = 1 - core
    each(
        even + quarter * role[2],
        side * (1 - role[3]),
        lambda i: greet(barrier, {"ep": base + lax.rem(spot * even + i, side)}),
    )

    @pl.when(role[1] == 1)
    def _():
        greet(barrier, {"ep": me - quarter})

    load_tok = pltpu.make_async_copy(tokens, tok, h_send.at[0])
    small = [
        pltpu.make_async_copy(src, dst, sem)
        for src, dst, sem in (
            (gain_h, gain, h_send.at[1]),
            (chosen_h, chosen, b_send.at[1]),
            (route_h, route, f_send.at[0]),
        )
    ]
    small[1].start()
    load_tok.start()
    small[0].start()
    small[2].start()
    ff = wd.shape[0]
    loads = [
        pltpu.make_async_copy(src.at[0], dst, sem)
        for src, dst, sem in (
            (gate_w, wgu.at[:, pl.ds(0, ff)], q_send.at[0]),
            (up_w, wgu.at[:, pl.ds(ff, ff)], q_send.at[1]),
            (down_w, wd, b_send.at[0]),
        )
    ]

    @pl.when(role[3] == 1)
    def _():
        pl.semaphore_wait(barrier, 1 + side)
        each(quarter, side, lambda i: greet(ready, {"ep": i}))

    with phase("load"):
        small[1].wait()
    picked = (chosen[...] - me * tok_rows).astype(f32)
    mine_rows = jnp.where(far_half == 1, picked[side:], picked[:side])

    def hot_rows(j):
        size = sizes[j]
        rows = side * 2 * size
        row = lax.broadcasted_iota(jnp.int32, (rows, slots), 0)
        lane = lax.broadcasted_iota(jnp.int32, (rows, slots), 1)
        value = jnp.zeros((rows, slots), f32)
        want = jnp.zeros((rows, slots), jnp.int32)
        for k in range(side):
            for h in range(2):
                at = (2 * k + h) * size
                here = row >= at
                if h == 0:
                    value = jnp.where(here, mine_rows[k : k + 1, :], value)
                want = jnp.where(here, row + (h * half + starts[j] - at), want)
        index = jnp.sum(jnp.where(lane == want, value, 0.0), axis=-1, keepdims=True)
        token = lax.broadcasted_iota(jnp.int32, (rows, tok_rows), 1).astype(f32)
        return jnp.where(token == index, 1.0, 0.0)

    def block_rows(b, count):
        at = b * count
        return pl.ds(at if isinstance(b, int) else pl.multiple_of(at, count), count)

    def pack(value, ref, j, b):
        count = value.shape[0]
        for s in range(pieces):
            flat[pl.ds(s, count, stride=pieces), :] = value[:, s * LANES : (s + 1) * LANES]
        packed = flat[: count * pieces, :].reshape(count, pieces, LANES)
        ref[j, block_rows(b, count)] = packed.astype(bf16)

    def gather(j):
        count = bunch * 2 * sizes[j]
        with phase("hot"):
            g_rows[: blocks * count, :] = hot_rows(j)
        if j == 0:
            with phase("tok"):
                load_tok.wait()
                small[0].wait()
            for load in loads:
                load.start()

        def one(b):
            hot = g_rows[block_rows(b, count), :].astype(bf16)
            with phase("norm"):
                got = jnp.dot(hot, tok[...], preferred_element_type=f32)
                scale = lax.rsqrt(jnp.mean(got * got, axis=-1, keepdims=True) + 1e-06)
                got = got * scale * gain[...].astype(f32).reshape(1, width)
            with phase("pack"):
                pack(got, out_x, j, b)

        loop(blocks, one)

    def dispatch(j, low, high):
        count = 2 * sizes[j]

        def one(i):
            k = lax.rem(spot * even + i, side)
            pltpu.make_async_remote_copy(
                src_ref=out_x.at[j, pl.ds(k * count, count)],
                dst_ref=in_x.at[2 * core + j, pl.ds(spot * count, count)],
                send_sem=d_send.at[j],
                recv_sem=d_recv.at[j],
                device_id={"ep": base + k},
                device_id_type=MESH,
            ).start()

        each(low, high, one)

    def part_rows(j, p):
        count = quarter * 2 * sizes[j]
        return pl.ds(p * count, count)

    def relay(j, p):
        return pltpu.make_async_remote_copy(
            src_ref=out_x.at[j, part_rows(j, p)],
            dst_ref=relay_x.at[j, part_rows(j, p)],
            send_sem=r_send.at[2 * j + p],
            recv_sem=r_recv.at[2 * j + p],
            device_id={"ep": me + quarter},
            device_id_type=MESH,
        )

    def pass_on(j, p):
        count = 2 * sizes[j]
        relay(j, p).wait_recv()

        def one(k):
            pltpu.make_async_remote_copy(
                src_ref=relay_x.at[j, pl.ds(k * count, count)],
                dst_ref=in_x.at[2 + j, pl.ds((spot - quarter) * count, count)],
                send_sem=h_send.at[j],
                recv_sem=d_recv.at[j],
                device_id={"ep": base + k},
                device_id_type=MESH,
            ).start()

        each(p * quarter, (p + 1) * quarter, one)

    def keep_dispatch(j):
        count = 2 * sizes[j]

        @pl.when(core == 0)
        def _():
            for r in range(count):
                in_x[j, spot * count + r] = out_x[j, spot * count + r]

    def rows_copy(src, dst, j, rows, send_sem, recv_sem):
        return pltpu.make_async_remote_copy(
            src_ref=src.at[j, pl.ds(0, rows)],
            dst_ref=dst.at[j, pl.ds(0, rows)],
            send_sem=send_sem.at[j],
            recv_sem=recv_sem.at[j],
            device_id=sib,
            device_id_type=MESH,
        )

    def by_core(rows_even, rows_odd, wait):
        @pl.when(core == 0)
        def _():
            wait(rows_even)

        @pl.when(core == 1)
        def _():
            wait(rows_odd)

    def dispatched(j):
        count = 2 * sizes[j]
        by_core(
            (side - 1) * count,
            side * count,
            lambda rows: rows_copy(out_x, in_x, j, rows, d_send, d_recv).wait_recv(),
        )

    def dispatch_left(j):
        count = 2 * sizes[j]

        @pl.when(core == 0)
        def _():
            rows_copy(out_x, in_x, j, (side - 1) * count, d_send, d_recv).wait_send()

        @pl.when(core - role[0] == 1)
        def _():
            rows_copy(out_x, in_x, j, side * count, d_send, d_recv).wait_send()

        @pl.when(role[0] == 1)
        def _():
            for p in range(2):
                relay(j, p).wait_send()

        @pl.when(role[1] == 1)
        def _():
            rows_copy(relay_x, in_x, j, side * count, h_send, d_recv).wait_send()

    def returned(j, sent):
        def wait(rows):
            copy = rows_copy(c_recv, c_recv, j, rows, b_send, b_recv)
            copy.wait_send() if sent else copy.wait_recv()

        by_core((n - 1) * sizes[j], n * sizes[j], wait)

    def forward(j):
        rows = pl.ds(0, side * 2 * sizes[j])
        return pltpu.make_async_remote_copy(
            src_ref=in_x.at[2 * core + j, rows],
            dst_ref=in_x.at[2 * core + j, rows],
            send_sem=f_send.at[j],
            recv_sem=f_recv.at[j],
            device_id=sib,
            device_id_type=MESH,
        )

    def even_sum(j):
        return 4 * upper if j == 0 else 1

    def own_sum(j):
        return core * (2 + j) + (1 - core) * even_sum(j)

    def swap(j):
        return pltpu.make_async_remote_copy(
            src_ref=sums.at[(1 - core) * (2 + j) + core * even_sum(j)],
            dst_ref=p_recv.at[j],
            send_sem=q_send.at[j],
            recv_sem=q_recv.at[j],
            device_id=sib,
            device_id_type=MESH,
        )

    def give_back(j):
        size = sizes[j]

        first = even * spot + (role[0] + role[1]) * quarter

        def one(i):
            k = lax.rem(first + i, side)
            for h in range(2):
                pltpu.make_async_remote_copy(
                    src_ref=c_send.at[j, pl.ds((2 * k + h) * size, size)],
                    dst_ref=c_recv.at[j, pl.ds(me * size, size)],
                    send_sem=b_send.at[j],
                    recv_sem=b_recv.at[j],
                    device_id={"ep": base + k, "tp": h},
                    device_id_type=MESH,
                ).start()

        each(even, side, one)

        @pl.when(core == 0)
        def _():
            pltpu.make_async_remote_copy(
                src_ref=c_send.at[j, pl.ds((2 * spot + 1) * size, size)],
                dst_ref=c_recv.at[j, pl.ds(me * size, size)],
                send_sem=b_send.at[j],
                recv_sem=b_recv.at[j],
                device_id=sib,
                device_id_type=MESH,
            ).start()
            for r in range(size):
                c_recv[j, me * size + r] = c_send[j, 2 * spot * size + r]

    def arrive(j):
        with phase(f"arrive{j}"):
            dispatched(j)
            forward(j).start()

    windows = [0, pad, pad + first_pad]

    def to_cols(index):
        j = index % 2
        count = bunch * 2 * sizes[j]
        at = windows[0 if index > 1 else 1 + j]

        def one(b):
            got = in_x[index, block_rows(b, count)].astype(f32)
            flat[pl.ds(0, count * pieces), :] = got.reshape(count * pieces, LANES)
            for s in range(pieces):
                x_cols[b, at : at + count, s * LANES : (s + 1) * LANES] = flat[
                    pl.ds(s, count, stride=pieces), :
                ].astype(bf16)

        loop(blocks, one)

    def experts_part(j):
        tiles = range(0, ff, TILE)

        def one(b):
            def both(c):
                gate = jnp.dot(x_cols[b], wgu[:, c : c + TILE], preferred_element_type=f32)
                up = jnp.dot(x_cols[b], wgu[:, ff + c : ff + c + TILE], preferred_element_type=f32)
                return gate, up

            total = None
            ahead = both(0)
            for c in tiles:
                gate, up = ahead
                if c + TILE < ff:
                    ahead = both(c + TILE)
                act = (gate / (1.0 + jnp.exp(-gate)) * up).astype(bf16)
                got = jnp.dot(act, wd[c : c + TILE, :], preferred_element_type=f32)
                total = got if total is None else total + got
            for window, k, index in ((0, j, 2 + j), (1, 0, 4 * j), (2, 1, 1)):
                if k <= j:
                    at, count = windows[window], bunch * 2 * sizes[k]
                    sums[index, b, :count] = total[at : at + count].astype(bf16)

        loop(blocks, one)

    def combine(j):
        count = bunch * 2 * sizes[j]

        def one(b):
            both = sums[own_sum(j), b, :count].astype(f32) + p_recv[j, b, :count].astype(f32)
            pack(both, c_send, j, b)

        loop(blocks, one)

    def finish(j):
        with phase(f"swap{j}"):
            swap(j).wait_recv()
        with phase(f"combine{j}"):
            combine(j)
            give_back(j)

    for j in chunks:
        with phase(f"gather{j}"):
            gather(j)
        if j == 0:

            with phase("enter"):

                @pl.when(role[3] == 0)
                def _():
                    entered = side * (1 - core) + 2 * role[0]
                    entered = entered + (1 + quarter) * role[1] + (1 + side) * role[2]
                    pl.semaphore_wait(barrier, entered)

        dispatch(j, even, side * (1 - role[0]) - quarter * role[1])
        keep_dispatch(j)

        @pl.when(role[0] == 1)
        def _():
            for p in (0, 1) if j == 0 else (1, 0):
                relay(j, p).start()

    small[2].wait()
    mine = (picked - core * half_rows).T
    weight = route[...].T
    lane = lax.broadcasted_iota(jnp.int32, (half, half_rows), 1).astype(f32)
    for e in range(experts):
        pair = [mine[h * half : (h + 1) * half, e : e + 1] for h in range(2)]
        row = jnp.where(core == 0, pair[0], pair[1])
        pair = [weight[h * half : (h + 1) * half, e : e + 1] for h in range(2)]
        share = jnp.where(core == 0, pair[0], pair[1])
        here = jnp.where(lane == row, share, 0.0)
        for j, size in enumerate(sizes):
            at = experts * starts[j] + e * size
            w_rows[at : at + size, :] = here[starts[j] : starts[j] + size]
    turned = w_rows[...].T
    high = turned.astype(bf16)
    spread[:half_rows, :] = high.astype(f32)
    spread[half_rows:, :] = turned - high.astype(f32)
    x_cols[...] = jnp.zeros(x_cols.shape, bf16)

    with phase("ready"):

        @pl.when(role[1] == 1)
        def _():
            pass_on(0, 0)
            pl.semaphore_wait(ready, quarter)
            dispatch(0, quarter, side)
            pass_on(0, 1)
            for j in chunks[1:]:
                dispatch(j, quarter, side)

    arrive(0)
    with phase("pass"):

        @pl.when(role[1] == 1)
        def _():
            for j in chunks[1:]:
                pass_on(j, 1)
                pass_on(j, 0)

    for load in loads[:2]:
        load.wait()
    last = 1
    lower = 1 - upper
    odd = core

    def when(flag, *steps):
        @pl.when(flag == 1)
        def _():
            for step, *args in steps:
                step(*args)

    def came(j):
        with phase(f"forward{j}"):
            forward(j).wait_recv()

    def send(j):
        swap(j).start()

    when(odd, (to_cols, 2))
    when(odd * lower, (came, 0))
    when(lower, (to_cols, 0))
    when(even, (came, 0), (to_cols, 2))
    loads[2].wait()
    with phase("down0"):
        experts_part(0)
    when(1 - odd * upper, (send, 0))
    arrive(1)
    when(odd, (to_cols, 3))
    when(even, (to_cols, 1))
    when(1 - even * upper, (finish, 0))
    when(odd * upper, (came, 0))
    when(upper, (to_cols, 0))
    came(1)
    when(odd, (to_cols, 1))
    when(even, (to_cols, 3))
    with phase("down1"):
        experts_part(1)
    when(odd * upper, (send, 0))
    send(1)
    when(even * upper, (finish, 0))

    with phase("left"):
        for j in chunks:
            dispatch_left(j)
            forward(j).wait_send()
    finish(last)
    with phase("left"):
        for j in chunks:
            swap(j).wait_send()
        for j in chunks[:last]:
            returned(j, True)

    for j in chunks:
        if j == last:
            returned(j, True)
        with phase(f"returned{j}"):
            returned(j, False)
        block = 8 * sizes[j]

        def unpack(b):
            got = c_recv[j, block_rows(b, block)].astype(f32)
            flat[: block * pieces, :] = got.reshape(block * pieces, LANES)
            at = experts * starts[j] + b * block
            at = at if isinstance(b, int) else pl.multiple_of(at, 8)
            for s in range(pieces):
                r_cols[pl.ds(at, block), s * LANES : (s + 1) * LANES] = flat[
                    pl.ds(s, block, stride=pieces), :
                ]

        loop(experts // 8, unpack)
    for k in range(2):
        part = slice(k * cols, (k + 1) * cols)
        res = r_cols[:, part].astype(bf16)
        total = jnp.dot(spread[...].astype(bf16), res, preferred_element_type=f32)
        mixed[:, part] = (total[:half_rows] + total[half_rows:]).astype(bf16)


def local(n, tokens, norm_gain, chosen_rows, route_weights, gate_weight, up_weight, down_weight):
    tok_rows, width = tokens.shape
    half_rows = tok_rows // 2
    experts, slots = chosen_rows.shape
    half = slots // 2
    rows = experts * half
    sizes = group_sizes(half)
    parts = len(sizes)
    top = max(sizes)
    side = n // 2
    bunch = min(side, 4)
    blocks = side // bunch
    block = bunch * 2 * top
    pad = round_up(block, 16)
    first_pad = round_up(bunch * 2 * sizes[0], 16)
    pieces = width // LANES
    ff = gate_weight.shape[2]
    bf16, f32 = jnp.bfloat16, jnp.float32
    packed = pltpu.VMEM((parts, n * top, pieces, LANES), bf16)
    vmem = pl.BlockSpec(memory_space=pltpu.VMEM)
    hbm = pl.BlockSpec(memory_space=pltpu.HBM)
    scratch = [
        pltpu.VMEM((tok_rows, width), bf16),
        pltpu.VMEM(norm_gain.shape, norm_gain.dtype),
        pltpu.VMEM(chosen_rows.shape, chosen_rows.dtype),
        pltpu.VMEM(route_weights.shape, route_weights.dtype),
        pltpu.VMEM((width, 2 * ff), bf16),
        pltpu.VMEM(down_weight.shape[1:], bf16),
        packed,
        pltpu.VMEM((4, n * top, pieces, LANES), bf16),
        packed,
        pltpu.VMEM((max(block, 8 * top) * pieces, LANES), f32),
        pltpu.VMEM((blocks, 2 * pad + first_pad, width), bf16),
        pltpu.VMEM((5, blocks, block, width), bf16),
        pltpu.VMEM((2, blocks, block, width), bf16),
        packed,
        packed,
        pltpu.VMEM((n * top, tok_rows), f32),
        pltpu.VMEM((rows, half_rows), f32),
        pltpu.VMEM((tok_rows, rows), f32),
        pltpu.VMEM((rows, width), f32),
    ]
    limit = VMEM_BYTES - half_rows * width * 2
    return pl.pallas_call(
        functools.partial(kernel, n),
        out_shape=pltpu.VMEM((half_rows, width), bf16),
        in_specs=[hbm] * 7,
        out_specs=vmem,
        scratch_shapes=scratch
        + [pltpu.SemaphoreType.DMA((parts,))] * 8
        + [pltpu.SemaphoreType.DMA((2 * parts,))] * 2
        + [pltpu.SemaphoreType.DMA((parts,))]
        + [pltpu.SemaphoreType.REGULAR],
        compiler_params=pltpu.CompilerParams(
            collective_id=0, has_side_effects=True, vmem_limit_bytes=limit
        ),
    )(
        tokens,
        norm_gain,
        chosen_rows,
        route_weights,
        gate_weight,
        up_weight,
        down_weight,
    )


def solution(mesh):
    return jax.shard_map(
        functools.partial(local, mesh.shape["ep"]),
        mesh=mesh,
        in_specs=(
            P(("grp", "ep"), None),
            P(),
            P("grp", "ep"),
            P("grp", "ep"),
            P("ep", None, "tp"),
            P("ep", None, "tp"),
            P("ep", "tp", None),
        ),
        out_specs=P(("grp", "ep", "tp"), None),
        check_vma=False,
    )
```

```python
import functools

import jax
import jax.numpy as jnp
from jax import lax
from jax.experimental import pallas as pl
from jax.experimental.pallas import tpu as pltpu
from jax.sharding import PartitionSpec as P

MESH = pl.DeviceIdType.MESH
LANES = 128
PARTS = 2
TILE = 256
VMEM_BYTES = 67043328


phase = jax.named_scope


def loop(count, body):
    if count == 1:
        body(0)
    else:
        lax.fori_loop(0, count, lambda i, carry: (body(i), carry)[1], 0)


def each(low, high, body):
    lax.fori_loop(low, high, lambda i, carry: (body(i), carry)[1], 0)


def group_sizes(half):
    base = half // PARTS
    sizes = [base + (1 if i >= PARTS - half % PARTS else 0) for i in range(PARTS)]
    return [s for s in sizes if s]


def round_up(a, b):
    return (a + b - 1) // b * b


def kernel(
    n,
    tokens,
    gain_h,
    chosen_h,
    route_h,
    gate_w,
    up_w,
    down_w,
    mixed,
    tok,
    gain,
    chosen,
    route,
    wgu,
    wd,
    out_x,
    in_x,
    relay_x,
    flat,
    x_cols,
    sums,
    p_recv,
    c_send,
    c_recv,
    g_rows,
    w_rows,
    pair_rows,
    spread_a,
    spread_b,
    held,
    r_cols,
    d_send,
    d_recv,
    f_send,
    f_recv,
    q_send,
    q_recv,
    b_send,
    b_recv,
    r_send,
    r_recv,
    h_send,
    ready,
):
    tok_rows, width = tok.shape
    half_rows = tok_rows // 2
    experts, slots = chosen.shape
    half = slots // 2
    sizes = group_sizes(half)
    starts = [sum(sizes[:j]) for j in range(len(sizes))]
    chunks = range(len(sizes))
    side = n // 2
    quarter = n // 4
    bunch = min(side, 4)
    blocks = side // bunch
    pad = round_up(bunch * 2 * max(sizes), 16)
    first_pad = round_up(bunch * 2 * sizes[0], 16)
    pieces = width // LANES
    cols = width // 2
    spread = [spread_a, spread_b]
    packed_rows = [round_up(experts * size, 16) for size in sizes]
    packed_at = [0, packed_rows[0]]
    f32, bf16 = jnp.float32, jnp.bfloat16
    me = lax.axis_index("ep")
    core = lax.axis_index("tp")
    sib = {"tp": 1 - core}
    upper = lax.div(me, side)
    spot = me - upper * side
    far_half = upper + core - 2 * upper * core
    base = far_half * side
    place = lax.div(me, quarter)
    role = [core * jnp.where(place == i, 1, 0) for i in range(4)]

    barrier = pltpu.get_barrier_semaphore()

    def greet(semaphore, target):
        pl.semaphore_signal(semaphore, inc=1, device_id=target, device_id_type=MESH)

    greet(barrier, sib)
    even = 1 - core
    each(
        even + quarter * role[2],
        side * (1 - role[3]),
        lambda i: greet(barrier, {"ep": base + lax.rem(spot * even + i, side)}),
    )

    @pl.when(role[1] == 1)
    def _():
        greet(barrier, {"ep": me - quarter})

    load_tok = pltpu.make_async_copy(tokens, tok, h_send)
    small = [
        pltpu.make_async_copy(src, dst, sem)
        for src, dst, sem in (
            (gain_h, gain, r_send),
            (chosen_h, chosen, d_send),
            (route_h, route, b_send.at[1]),
        )
    ]
    small[1].start()
    load_tok.start()
    small[0].start()
    small[2].start()
    ff = wd.shape[0]
    loads = [
        pltpu.make_async_copy(src.at[0], dst, sem)
        for src, dst, sem in (
            (gate_w, wgu.at[:, pl.ds(0, ff)], q_send),
            (up_w, wgu.at[:, pl.ds(ff, ff)], f_send),
            (down_w, wd, b_send.at[0]),
        )
    ]

    @pl.when(role[3] == 1)
    def _():
        pl.semaphore_wait(barrier, 1 + side)
        each(quarter, side, lambda i: greet(ready, {"ep": i}))

    with phase("load"):
        small[1].wait()
    picked = (chosen[...] - me * tok_rows).astype(f32)
    mine_rows = jnp.where(far_half == 1, picked[side:], picked[:side])

    def hot_rows(j):
        size = sizes[j]
        rows = side * 2 * size
        row = lax.broadcasted_iota(jnp.int32, (rows, slots), 0)
        lane = lax.broadcasted_iota(jnp.int32, (rows, slots), 1)
        value = jnp.zeros((rows, slots), f32)
        want = jnp.zeros((rows, slots), jnp.int32)
        for k in range(side):
            for h in range(2):
                at = (2 * k + h) * size
                here = row >= at
                if h == 0:
                    value = jnp.where(here, mine_rows[k : k + 1, :], value)
                want = jnp.where(here, row + (h * half + starts[j] - at), want)
        index = jnp.sum(jnp.where(lane == want, value, 0.0), axis=-1, keepdims=True)
        token = lax.broadcasted_iota(jnp.int32, (rows, tok_rows), 1).astype(f32)
        return jnp.where(token == index, 1.0, 0.0)

    def block_rows(b, count):
        at = b * count
        return pl.ds(at if isinstance(b, int) else pl.multiple_of(at, count), count)

    def pack(value, ref, j, b):
        count = value.shape[0]
        for s in range(pieces):
            flat[pl.ds(s, count, stride=pieces), :] = value[:, s * LANES : (s + 1) * LANES]
        packed = flat[: count * pieces, :].reshape(count, pieces, LANES)
        ref[j, block_rows(b, count)] = packed.astype(bf16)

    def gather(j):
        count = bunch * 2 * sizes[j]
        with phase("hot"):
            g_rows[: blocks * count, :] = hot_rows(j)
        if j == 0:
            with phase("tok"):
                load_tok.wait()
                small[0].wait()
            for load in loads:
                load.start()

        def one(b):
            hot = g_rows[block_rows(b, count), :].astype(bf16)
            with phase("norm"):
                got = jnp.dot(hot, tok[...], preferred_element_type=f32)
                scale = lax.rsqrt(jnp.mean(got * got, axis=-1, keepdims=True) + 1e-06)
                got = got * scale * gain[...].astype(f32).reshape(1, width)
            with phase("pack"):
                pack(got, out_x, j, b)

        loop(blocks, one)

    def dispatch(j, low, high):
        count = 2 * sizes[j]

        def one(i):
            k = lax.rem(spot * even + i, side)
            pltpu.make_async_remote_copy(
                src_ref=out_x.at[j, pl.ds(k * count, count)],
                dst_ref=in_x.at[2 * core + j, pl.ds(spot * count, count)],
                send_sem=d_send,
                recv_sem=d_recv.at[j],
                device_id={"ep": base + k},
                device_id_type=MESH,
            ).start()

        each(low, high, one)

    def part_rows(j, p):
        count = quarter * 2 * sizes[j]
        return pl.ds(p * count, count)

    def relay(j, p):
        return pltpu.make_async_remote_copy(
            src_ref=out_x.at[j, part_rows(j, p)],
            dst_ref=relay_x.at[j, part_rows(j, p)],
            send_sem=r_send,
            recv_sem=r_recv.at[2 * j + p],
            device_id={"ep": me + quarter},
            device_id_type=MESH,
        )

    def pass_on(j, p):
        count = 2 * sizes[j]
        relay(j, p).wait_recv()

        def one(k):
            pltpu.make_async_remote_copy(
                src_ref=relay_x.at[j, pl.ds(k * count, count)],
                dst_ref=in_x.at[2 + j, pl.ds((spot - quarter) * count, count)],
                send_sem=h_send,
                recv_sem=d_recv.at[j],
                device_id={"ep": base + k},
                device_id_type=MESH,
            ).start()

        each(p * quarter, (p + 1) * quarter, one)

    def keep_dispatch(j):
        count = 2 * sizes[j]

        @pl.when(core == 0)
        def _():
            for r in range(count):
                in_x[j, spot * count + r] = out_x[j, spot * count + r]

    def rows_copy(src, dst, j, rows, send_sem, recv_sem):
        return pltpu.make_async_remote_copy(
            src_ref=src.at[j, pl.ds(0, rows)],
            dst_ref=dst.at[j, pl.ds(0, rows)],
            send_sem=send_sem,
            recv_sem=recv_sem,
            device_id=sib,
            device_id_type=MESH,
        )

    def by_core(rows_even, rows_odd, wait):
        @pl.when(core == 0)
        def _():
            wait(rows_even)

        @pl.when(core == 1)
        def _():
            wait(rows_odd)

    def dispatched(j):
        count = 2 * sizes[j]
        by_core(
            (side - 1) * count,
            side * count,
            lambda rows: rows_copy(out_x, in_x, j, rows, d_send, d_recv.at[j]).wait_recv(),
        )

    def both_chunks(ref, rows):
        return ref.at[pl.ds(0, 2), pl.ds(0, rows)]

    def sent(ref, semaphore):
        pltpu.make_async_remote_copy(
            src_ref=ref,
            dst_ref=ref,
            send_sem=semaphore,
            recv_sem=d_recv.at[0],
            device_id=sib,
            device_id_type=MESH,
        ).wait_send()

    def dispatch_left():
        @pl.when(core == 0)
        def _():
            sent(both_chunks(out_x, (side - 1) * half), d_send)

        @pl.when(core - role[0] == 1)
        def _():
            sent(both_chunks(out_x, side * half), d_send)

        @pl.when(role[0] == 1)
        def _():
            sent(both_chunks(out_x, side * half), r_send)

        @pl.when(role[1] == 1)
        def _():
            sent(both_chunks(relay_x, side * half), h_send)

    def returned(j, left):
        def wait(rows):
            copy = rows_copy(c_recv, c_recv, j, rows, b_send.at[j], b_recv.at[j])
            copy.wait_send() if left else copy.wait_recv()

        by_core((n - 1) * sizes[j], n * sizes[j], wait)

    def forward(j):
        rows = pl.ds(0, side * 2 * sizes[j])
        return pltpu.make_async_remote_copy(
            src_ref=in_x.at[2 * core + j, rows],
            dst_ref=in_x.at[2 * core + j, rows],
            send_sem=f_send,
            recv_sem=f_recv.at[j],
            device_id=sib,
            device_id_type=MESH,
        )

    def even_sum(j):
        return 4 * upper if j == 0 else 1

    def own_sum(j):
        return core * (2 + j) + (1 - core) * even_sum(j)

    def swap(j):
        return pltpu.make_async_remote_copy(
            src_ref=sums.at[(1 - core) * (2 + j) + core * even_sum(j)],
            dst_ref=p_recv.at[j],
            send_sem=q_send,
            recv_sem=q_recv.at[j],
            device_id=sib,
            device_id_type=MESH,
        )

    def give_back(j):
        size = sizes[j]

        first = even * spot + (role[0] + role[1]) * quarter

        def one(i):
            k = lax.rem(first + i, side)
            for h in range(2):
                pltpu.make_async_remote_copy(
                    src_ref=c_send.at[j, pl.ds((2 * k + h) * size, size)],
                    dst_ref=c_recv.at[j, pl.ds(me * size, size)],
                    send_sem=b_send.at[j],
                    recv_sem=b_recv.at[j],
                    device_id={"ep": base + k, "tp": h},
                    device_id_type=MESH,
                ).start()

        each(even, side, one)

        @pl.when(core == 0)
        def _():
            pltpu.make_async_remote_copy(
                src_ref=c_send.at[j, pl.ds((2 * spot + 1) * size, size)],
                dst_ref=c_recv.at[j, pl.ds(me * size, size)],
                send_sem=b_send.at[j],
                recv_sem=b_recv.at[j],
                device_id=sib,
                device_id_type=MESH,
            ).start()
            for r in range(size):
                c_recv[j, me * size + r] = c_send[j, 2 * spot * size + r]

    def arrive(j):
        with phase(f"arrive{j}"):
            dispatched(j)
            forward(j).start()

    windows = [0, pad, pad + first_pad]

    def to_cols(index):
        j = index % 2
        count = bunch * 2 * sizes[j]
        at = windows[0 if index > 1 else 1 + j]

        def one(b):
            got = in_x[index, block_rows(b, count)].astype(f32)
            flat[pl.ds(0, count * pieces), :] = got.reshape(count * pieces, LANES)
            for s in range(pieces):
                x_cols[b, at : at + count, s * LANES : (s + 1) * LANES] = flat[
                    pl.ds(s, count, stride=pieces), :
                ].astype(bf16)

        loop(blocks, one)

    def experts_part(j):
        tiles = range(0, ff, TILE)

        def one(b):
            def both(c):
                gate = jnp.dot(x_cols[b], wgu[:, c : c + TILE], preferred_element_type=f32)
                up = jnp.dot(x_cols[b], wgu[:, ff + c : ff + c + TILE], preferred_element_type=f32)
                return gate, up

            total = None
            ahead = both(0)
            for c in tiles:
                gate, up = ahead
                if c + TILE < ff:
                    ahead = both(c + TILE)
                act = (gate / (1.0 + jnp.exp(-gate)) * up).astype(bf16)
                got = jnp.dot(act, wd[c : c + TILE, :], preferred_element_type=f32)
                total = got if total is None else total + got
            for window, k, index in ((0, j, 2 + j), (1, 0, 4 * j), (2, 1, 1)):
                if k <= j:
                    at, count = windows[window], bunch * 2 * sizes[k]
                    sums[index, b, :count] = total[at : at + count].astype(bf16)

        loop(blocks, one)

    def combine(j):
        count = bunch * 2 * sizes[j]

        def one(b):
            both = sums[own_sum(j), b, :count].astype(f32) + p_recv[j, b, :count].astype(f32)
            pack(both, c_send, j, b)

        loop(blocks, one)

    def finish(j):
        with phase(f"swap{j}"):
            swap(j).wait_recv()
        with phase(f"combine{j}"):
            combine(j)
            give_back(j)

    for j in chunks:
        with phase(f"gather{j}"):
            gather(j)
        if j == 0:

            with phase("enter"):

                @pl.when(role[3] == 0)
                def _():
                    entered = side * (1 - core) + 2 * role[0]
                    entered = entered + (1 + quarter) * role[1] + (1 + side) * role[2]
                    pl.semaphore_wait(barrier, entered)

        dispatch(j, even, side * (1 - role[0]) - quarter * role[1])
        keep_dispatch(j)

        @pl.when(role[0] == 1)
        def _():
            for p in (0, 1):
                relay(j, p).start()

    small[2].wait()
    mine = (picked - core * half_rows).T
    weight = route[...].T
    lane = lax.broadcasted_iota(jnp.int32, (half, half_rows), 1).astype(f32)
    w_rows[...] = jnp.zeros(w_rows.shape, f32)
    r_cols[...] = jnp.zeros(r_cols.shape, f32)
    for e in range(experts):
        pair = [mine[h * half : (h + 1) * half, e : e + 1] for h in range(2)]
        row = jnp.where(core == 0, pair[0], pair[1])
        pair = [weight[h * half : (h + 1) * half, e : e + 1] for h in range(2)]
        share = jnp.where(core == 0, pair[0], pair[1])
        here = jnp.where(lane == row, share, 0.0)
        for j, size in enumerate(sizes):
            at = packed_at[j] + e * size
            w_rows[at : at + size, :] = here[starts[j] : starts[j] + size]
    for j in chunks:
        some = packed_rows[j]
        value = w_rows[packed_at[j] : packed_at[j] + some, :]
        high = value.astype(bf16).astype(f32)
        pair_rows[:some, :] = high
        pair_rows[some : 2 * some, :] = value - high
        spread[j][...] = pair_rows[: 2 * some, :].T
    x_cols[...] = jnp.zeros(x_cols.shape, bf16)

    with phase("ready"):

        @pl.when(role[1] == 1)
        def _():
            pass_on(0, 0)
            pl.semaphore_wait(ready, quarter)
            dispatch(0, quarter, side)
            pass_on(0, 1)
            for j in chunks[1:]:
                dispatch(j, quarter, side)
                pass_on(j, 0)

    for load in loads[:2]:
        load.wait()
    arrive(0)
    with phase("pass"):

        @pl.when(role[1] == 1)
        def _():
            for j in chunks[1:]:
                pass_on(j, 1)

    last = 1
    lower = 1 - upper
    odd = core

    def when(flag, *steps):
        @pl.when(flag == 1)
        def _():
            for step, *args in steps:
                step(*args)

    def came(j):
        with phase(f"forward{j}"):
            forward(j).wait_recv()

    def send(j):
        swap(j).start()

    when(odd, (to_cols, 2))
    when(odd * lower, (came, 0))
    when(lower, (to_cols, 0))
    when(even, (came, 0), (to_cols, 2))
    loads[2].wait()
    with phase("down0"):
        experts_part(0)
    when(1 - odd * upper, (send, 0))
    arrive(1)
    when(odd, (to_cols, 3))
    when(even, (to_cols, 1))
    when(1 - even * upper, (finish, 0))
    when(odd * upper, (came, 0))
    when(upper, (to_cols, 0))
    came(1)
    when(odd, (to_cols, 1))
    when(even, (to_cols, 3))
    with phase("down1"):
        experts_part(1)
    when(odd * upper, (send, 0))
    send(1)
    when(even * upper, (finish, 0))

    with phase("left"):
        dispatch_left()
        sent(both_chunks(in_x, side * half), f_send)
    finish(last)
    with phase("left"):
        sent(sums.at[pl.ds(0, 2)], q_send)
        returned(0, True)

    for j in chunks:
        if j == last:
            returned(j, True)
        with phase(f"returned{j}"):
            returned(j, False)
        block = 8 * sizes[j]

        def unpack(b):
            got = c_recv[j, block_rows(b, block)].astype(f32)
            flat[: block * pieces, :] = got.reshape(block * pieces, LANES)
            at = packed_at[j] + b * block
            at = at if isinstance(b, int) else pl.multiple_of(at, 8)
            for s in range(pieces):
                r_cols[pl.ds(at, block), s * LANES : (s + 1) * LANES] = flat[
                    pl.ds(s, block, stride=pieces), :
                ]

        loop(experts // 8, unpack)
        here = slice(packed_at[j], packed_at[j] + packed_rows[j])
        for k in range(2):
            part = slice(k * cols, (k + 1) * cols)
            res = r_cols[here, part].astype(bf16)
            twice = jnp.concatenate([res, res], axis=0)
            total = jnp.dot(spread[j][...].astype(bf16), twice, preferred_element_type=f32)
            if j == 0:
                held[:, part] = total
            else:
                mixed[:, part] = (held[:, part] + total).astype(bf16)


def local(n, tokens, norm_gain, chosen_rows, route_weights, gate_weight, up_weight, down_weight):
    tok_rows, width = tokens.shape
    half_rows = tok_rows // 2
    experts, slots = chosen_rows.shape
    half = slots // 2
    sizes = group_sizes(half)
    packed_rows = [round_up(experts * size, 16) for size in sizes]
    parts = len(sizes)
    top = max(sizes)
    side = n // 2
    bunch = min(side, 4)
    blocks = side // bunch
    block = bunch * 2 * top
    pad = round_up(block, 16)
    first_pad = round_up(bunch * 2 * sizes[0], 16)
    pieces = width // LANES
    ff = gate_weight.shape[2]
    bf16, f32 = jnp.bfloat16, jnp.float32
    packed = pltpu.VMEM((parts, n * top, pieces, LANES), bf16)
    vmem = pl.BlockSpec(memory_space=pltpu.VMEM)
    hbm = pl.BlockSpec(memory_space=pltpu.HBM)
    scratch = [
        pltpu.VMEM((tok_rows, width), bf16),
        pltpu.VMEM(norm_gain.shape, norm_gain.dtype),
        pltpu.VMEM(chosen_rows.shape, chosen_rows.dtype),
        pltpu.VMEM(route_weights.shape, route_weights.dtype),
        pltpu.VMEM((width, 2 * ff), bf16),
        pltpu.VMEM(down_weight.shape[1:], bf16),
        packed,
        pltpu.VMEM((4, n * top, pieces, LANES), bf16),
        packed,
        pltpu.VMEM((max(block, 8 * top) * pieces, LANES), f32),
        pltpu.VMEM((blocks, 2 * pad + first_pad, width), bf16),
        pltpu.VMEM((5, blocks, block, width), bf16),
        pltpu.VMEM((2, blocks, block, width), bf16),
        packed,
        packed,
        pltpu.VMEM((n * top, tok_rows), f32),
        pltpu.VMEM((sum(packed_rows), half_rows), f32),
        pltpu.VMEM((2 * max(packed_rows), half_rows), f32),
        pltpu.VMEM((half_rows, 2 * packed_rows[0]), f32),
        pltpu.VMEM((half_rows, 2 * packed_rows[1]), f32),
        pltpu.VMEM((half_rows, width), f32),
        pltpu.VMEM((sum(packed_rows), width), f32),
    ]
    limit = VMEM_BYTES - half_rows * width * 2
    return pl.pallas_call(
        functools.partial(kernel, n),
        out_shape=pltpu.VMEM((half_rows, width), bf16),
        in_specs=[hbm] * 7,
        out_specs=vmem,
        scratch_shapes=scratch
        + [pltpu.SemaphoreType.DMA, pltpu.SemaphoreType.DMA((parts,))] * 3
        + [pltpu.SemaphoreType.DMA((parts,))] * 2
        + [pltpu.SemaphoreType.DMA, pltpu.SemaphoreType.DMA((2 * parts,)), pltpu.SemaphoreType.DMA]
        + [pltpu.SemaphoreType.REGULAR],
        compiler_params=pltpu.CompilerParams(
            collective_id=0, has_side_effects=True, vmem_limit_bytes=limit
        ),
    )(
        tokens,
        norm_gain,
        chosen_rows,
        route_weights,
        gate_weight,
        up_weight,
        down_weight,
    )


def solution(mesh):
    return jax.shard_map(
        functools.partial(local, mesh.shape["ep"]),
        mesh=mesh,
        in_specs=(
            P(("grp", "ep"), None),
            P(),
            P("grp", "ep"),
            P("grp", "ep"),
            P("ep", None, "tp"),
            P("ep", None, "tp"),
            P("ep", "tp", None),
        ),
        out_specs=P(("grp", "ep", "tp"), None),
        check_vma=False,
    )
```

```python
import functools

import jax
import jax.numpy as jnp
from jax import lax
from jax.experimental import pallas as pl
from jax.experimental.pallas import tpu as pltpu
from jax.sharding import PartitionSpec as P

MESH = pl.DeviceIdType.MESH
LANES = 128
PARTS = 2
TILE = 256
VMEM_BYTES = 67043328


phase = jax.named_scope


def loop(count, body):
    if count == 1:
        body(0)
    else:
        lax.fori_loop(0, count, lambda i, carry: (body(i), carry)[1], 0)


def each(low, high, body):
    lax.fori_loop(low, high, lambda i, carry: (body(i), carry)[1], 0)


def group_sizes(half):
    base = half // PARTS
    sizes = [base + (1 if i >= PARTS - half % PARTS else 0) for i in range(PARTS)]
    return [s for s in sizes if s]


def round_up(a, b):
    return (a + b - 1) // b * b


def kernel(
    n,
    tokens,
    gain_h,
    chosen_h,
    route_h,
    gate_w,
    up_w,
    down_w,
    mixed,
    tok,
    gain,
    chosen,
    route,
    wgu,
    wd,
    out_x,
    in_x,
    relay_x,
    flat,
    x_cols,
    sums,
    p_recv,
    c_send,
    c_recv,
    g_rows,
    w_rows,
    pair_rows,
    spread_a,
    spread_b,
    held,
    r_cols,
    d_send,
    d_recv,
    f_send,
    f_recv,
    q_send,
    q_recv,
    b_send,
    b_recv,
    r_send,
    r_recv,
    h_send,
    ready,
):
    tok_rows, width = tok.shape
    half_rows = tok_rows // 2
    experts, slots = chosen.shape
    half = slots // 2
    sizes = group_sizes(half)
    starts = [sum(sizes[:j]) for j in range(len(sizes))]
    chunks = range(len(sizes))
    side = n // 2
    quarter = n // 4
    bunch = min(side, 4)
    blocks = side // bunch
    pad = round_up(bunch * 2 * max(sizes), 16)
    first_pad = round_up(bunch * 2 * sizes[0], 16)
    pieces = width // LANES
    cols = width // 2
    spread = [spread_a, spread_b]
    packed_rows = [round_up(experts * size, 16) for size in sizes]
    packed_at = [0, packed_rows[0]]
    f32, bf16 = jnp.float32, jnp.bfloat16
    me = lax.axis_index("ep")
    core = lax.axis_index("tp")
    sib = {"tp": 1 - core}
    upper = lax.div(me, side)
    spot = me - upper * side
    far_half = upper + core - 2 * upper * core
    base = far_half * side
    place = lax.div(me, quarter)
    role = [core * jnp.where(place == i, 1, 0) for i in range(4)]

    barrier = pltpu.get_barrier_semaphore()

    def greet(semaphore, target):
        pl.semaphore_signal(semaphore, inc=1, device_id=target, device_id_type=MESH)

    even = 1 - core
    lower_odd = role[0] + role[1]
    each(
        even + quarter * role[2],
        side * (1 - role[3]),
        lambda i: greet(
            barrier,
            {"ep": base + lax.rem(spot * even + i + lower_odd * (side - 1 - 2 * i), side)},
        ),
    )
    greet(barrier, sib)

    @pl.when(role[1] == 1)
    def _():
        greet(barrier, {"ep": me - quarter})

    load_tok = pltpu.make_async_copy(tokens, tok, h_send)
    small = [
        pltpu.make_async_copy(src, dst, sem)
        for src, dst, sem in (
            (gain_h, gain, r_send),
            (chosen_h, chosen, d_send),
            (route_h, route, b_send.at[1]),
        )
    ]
    small[1].start()
    load_tok.start()
    small[0].start()
    small[2].start()
    ff = wd.shape[0]
    loads = [
        pltpu.make_async_copy(src.at[0], dst, sem)
        for src, dst, sem in (
            (gate_w, wgu.at[:, pl.ds(0, ff)], q_send),
            (up_w, wgu.at[:, pl.ds(ff, ff)], f_send),
            (down_w, wd, b_send.at[0]),
        )
    ]

    @pl.when(role[3] == 1)
    def _():
        pl.semaphore_wait(barrier, 1 + side)
        each(quarter, side, lambda i: greet(ready, {"ep": i}))

    with phase("load"):
        small[1].wait()
    picked = (chosen[...] - me * tok_rows).astype(f32)
    mine_rows = jnp.where(far_half == 1, picked[side:], picked[:side])

    def hot_rows(j):
        size = sizes[j]
        rows = side * 2 * size
        row = lax.broadcasted_iota(jnp.int32, (rows, slots), 0)
        lane = lax.broadcasted_iota(jnp.int32, (rows, slots), 1)
        value = jnp.zeros((rows, slots), f32)
        want = jnp.zeros((rows, slots), jnp.int32)
        for k in range(side):
            for h in range(2):
                at = (2 * k + h) * size
                here = row >= at
                if h == 0:
                    value = jnp.where(here, mine_rows[k : k + 1, :], value)
                want = jnp.where(here, row + (h * half + starts[j] - at), want)
        index = jnp.sum(jnp.where(lane == want, value, 0.0), axis=-1, keepdims=True)
        token = lax.broadcasted_iota(jnp.int32, (rows, tok_rows), 1).astype(f32)
        return jnp.where(token == index, 1.0, 0.0)

    def block_rows(b, count):
        at = b * count
        return pl.ds(at if isinstance(b, int) else pl.multiple_of(at, count), count)

    def pack(value, ref, j, b):
        count = value.shape[0]
        for s in range(pieces):
            flat[pl.ds(s, count, stride=pieces), :] = value[:, s * LANES : (s + 1) * LANES]
        packed = flat[: count * pieces, :].reshape(count, pieces, LANES)
        ref[j, block_rows(b, count)] = packed.astype(bf16)

    def gather(j):
        count = bunch * 2 * sizes[j]
        with phase("hot"):
            g_rows[: blocks * count, :] = hot_rows(j)
        if j == 0:
            with phase("tok"):
                load_tok.wait()
                small[0].wait()
            for load in loads:
                load.start()

        def one(b):
            hot = g_rows[block_rows(b, count), :].astype(bf16)
            with phase("norm"):
                got = jnp.dot(hot, tok[...], preferred_element_type=f32)
                scale = lax.rsqrt(jnp.mean(got * got, axis=-1, keepdims=True) + 1e-06)
                got = got * scale * gain[...].astype(f32).reshape(1, width)
            with phase("pack"):
                pack(got, out_x, j, b)

        loop(blocks, one)

    def dispatch(j, low, high):
        count = 2 * sizes[j]

        def one(i):
            k = lax.rem(spot * even + i, side)
            pltpu.make_async_remote_copy(
                src_ref=out_x.at[j, pl.ds(k * count, count)],
                dst_ref=in_x.at[2 * core + j, pl.ds(spot * count, count)],
                send_sem=d_send,
                recv_sem=d_recv.at[j],
                device_id={"ep": base + k},
                device_id_type=MESH,
            ).start()

        each(low, high, one)

    def part_rows(j, p):
        count = quarter * 2 * sizes[j]
        return pl.ds(p * count, count)

    def relay(j, p):
        return pltpu.make_async_remote_copy(
            src_ref=out_x.at[j, part_rows(j, p)],
            dst_ref=relay_x.at[j, part_rows(j, p)],
            send_sem=r_send,
            recv_sem=r_recv.at[2 * j + p],
            device_id={"ep": me + quarter},
            device_id_type=MESH,
        )

    def pass_on(j, p):
        count = 2 * sizes[j]
        relay(j, p).wait_recv()

        def one(k):
            pltpu.make_async_remote_copy(
                src_ref=relay_x.at[j, pl.ds(k * count, count)],
                dst_ref=in_x.at[2 + j, pl.ds((spot - quarter) * count, count)],
                send_sem=h_send,
                recv_sem=d_recv.at[j],
                device_id={"ep": base + k},
                device_id_type=MESH,
            ).start()

        each(p * quarter, (p + 1) * quarter, one)

    def keep_dispatch(j):
        count = 2 * sizes[j]

        @pl.when(core == 0)
        def _():
            for r in range(count):
                in_x[j, spot * count + r] = out_x[j, spot * count + r]

    def rows_copy(src, dst, j, rows, send_sem, recv_sem):
        return pltpu.make_async_remote_copy(
            src_ref=src.at[j, pl.ds(0, rows)],
            dst_ref=dst.at[j, pl.ds(0, rows)],
            send_sem=send_sem,
            recv_sem=recv_sem,
            device_id=sib,
            device_id_type=MESH,
        )

    def by_core(rows_even, rows_odd, wait):
        @pl.when(core == 0)
        def _():
            wait(rows_even)

        @pl.when(core == 1)
        def _():
            wait(rows_odd)

    def dispatched(j):
        count = 2 * sizes[j]
        by_core(
            (side - 1) * count,
            side * count,
            lambda rows: rows_copy(out_x, in_x, j, rows, d_send, d_recv.at[j]).wait_recv(),
        )

    def both_chunks(ref, rows):
        return ref.at[pl.ds(0, 2), pl.ds(0, rows)]

    def sent(ref, semaphore):
        pltpu.make_async_remote_copy(
            src_ref=ref,
            dst_ref=ref,
            send_sem=semaphore,
            recv_sem=d_recv.at[0],
            device_id=sib,
            device_id_type=MESH,
        ).wait_send()

    def dispatch_left():
        @pl.when(core == 0)
        def _():
            sent(both_chunks(out_x, (side - 1) * half), d_send)

        @pl.when(core - role[0] == 1)
        def _():
            sent(both_chunks(out_x, side * half), d_send)

        @pl.when(role[0] == 1)
        def _():
            sent(both_chunks(out_x, side * half), r_send)

        @pl.when(role[1] == 1)
        def _():
            sent(both_chunks(relay_x, side * half), h_send)

    def returned(j, left):
        def wait(rows):
            copy = rows_copy(c_recv, c_recv, j, rows, b_send.at[j], b_recv.at[j])
            copy.wait_send() if left else copy.wait_recv()

        by_core((n - 1) * sizes[j], n * sizes[j], wait)

    def forward(j):
        rows = pl.ds(0, side * 2 * sizes[j])
        return pltpu.make_async_remote_copy(
            src_ref=in_x.at[2 * core + j, rows],
            dst_ref=in_x.at[2 * core + j, rows],
            send_sem=f_send,
            recv_sem=f_recv.at[j],
            device_id=sib,
            device_id_type=MESH,
        )

    def even_sum(j):
        return 4 * upper if j == 0 else 1

    def own_sum(j):
        return core * (2 + j) + (1 - core) * even_sum(j)

    def swap(j):
        return pltpu.make_async_remote_copy(
            src_ref=sums.at[(1 - core) * (2 + j) + core * even_sum(j)],
            dst_ref=p_recv.at[j],
            send_sem=q_send,
            recv_sem=q_recv.at[j],
            device_id=sib,
            device_id_type=MESH,
        )

    def give_back(j):
        size = sizes[j]

        first = even * spot + (role[0] + role[1]) * quarter

        def one(i):
            k = lax.rem(first + i, side)
            for h in range(2):
                pltpu.make_async_remote_copy(
                    src_ref=c_send.at[j, pl.ds((2 * k + h) * size, size)],
                    dst_ref=c_recv.at[j, pl.ds(me * size, size)],
                    send_sem=b_send.at[j],
                    recv_sem=b_recv.at[j],
                    device_id={"ep": base + k, "tp": h},
                    device_id_type=MESH,
                ).start()

        each(even, side, one)

        @pl.when(core == 0)
        def _():
            pltpu.make_async_remote_copy(
                src_ref=c_send.at[j, pl.ds((2 * spot + 1) * size, size)],
                dst_ref=c_recv.at[j, pl.ds(me * size, size)],
                send_sem=b_send.at[j],
                recv_sem=b_recv.at[j],
                device_id=sib,
                device_id_type=MESH,
            ).start()
            for r in range(size):
                c_recv[j, me * size + r] = c_send[j, 2 * spot * size + r]

    def arrive(j):
        with phase(f"arrive{j}"):
            dispatched(j)
            forward(j).start()

    windows = [0, pad, pad + first_pad]

    def to_cols(index):
        j = index % 2
        count = bunch * 2 * sizes[j]
        at = windows[0 if index > 1 else 1 + j]

        def one(b):
            got = in_x[index, block_rows(b, count)].astype(f32)
            flat[pl.ds(0, count * pieces), :] = got.reshape(count * pieces, LANES)
            for s in range(pieces):
                x_cols[b, at : at + count, s * LANES : (s + 1) * LANES] = flat[
                    pl.ds(s, count, stride=pieces), :
                ].astype(bf16)

        loop(blocks, one)

    def experts_part(j):
        tiles = range(0, ff, TILE)

        def one(b):
            def both(c):
                gate = jnp.dot(x_cols[b], wgu[:, c : c + TILE], preferred_element_type=f32)
                up = jnp.dot(x_cols[b], wgu[:, ff + c : ff + c + TILE], preferred_element_type=f32)
                return gate, up

            total = None
            ahead = both(0)
            for c in tiles:
                gate, up = ahead
                if c + TILE < ff:
                    ahead = both(c + TILE)
                act = (gate / (1.0 + jnp.exp(-gate)) * up).astype(bf16)
                got = jnp.dot(act, wd[c : c + TILE, :], preferred_element_type=f32)
                total = got if total is None else total + got
            for window, k, index in ((0, j, 2 + j), (1, 0, 4 * j), (2, 1, 1)):
                if k <= j:
                    at, count = windows[window], bunch * 2 * sizes[k]
                    sums[index, b, :count] = total[at : at + count].astype(bf16)

        loop(blocks, one)

    def combine(j):
        count = bunch * 2 * sizes[j]

        def one(b):
            both = sums[own_sum(j), b, :count].astype(f32) + p_recv[j, b, :count].astype(f32)
            pack(both, c_send, j, b)

        loop(blocks, one)

    def finish(j):
        with phase(f"swap{j}"):
            swap(j).wait_recv()
        with phase(f"combine{j}"):
            combine(j)
            give_back(j)

    for j in chunks:
        with phase(f"gather{j}"):
            gather(j)
        if j == 0:

            with phase("enter"):

                @pl.when(role[3] == 0)
                def _():
                    entered = side * (1 - core) + 2 * role[0]
                    entered = entered + (1 + quarter) * role[1] + (1 + side) * role[2]
                    pl.semaphore_wait(barrier, entered)

        dispatch(j, even, side * (1 - role[0]) - quarter * role[1])
        keep_dispatch(j)

        @pl.when(role[0] == 1)
        def _():
            for p in (0, 1):
                relay(j, p).start()

    small[2].wait()
    mine = (picked - core * half_rows).T
    weight = route[...].T
    lane = lax.broadcasted_iota(jnp.int32, (half, half_rows), 1).astype(f32)
    w_rows[...] = jnp.zeros(w_rows.shape, f32)
    r_cols[...] = jnp.zeros(r_cols.shape, f32)
    for e in range(experts):
        pair = [mine[h * half : (h + 1) * half, e : e + 1] for h in range(2)]
        row = jnp.where(core == 0, pair[0], pair[1])
        pair = [weight[h * half : (h + 1) * half, e : e + 1] for h in range(2)]
        share = jnp.where(core == 0, pair[0], pair[1])
        here = jnp.where(lane == row, share, 0.0)
        for j, size in enumerate(sizes):
            at = packed_at[j] + e * size
            w_rows[at : at + size, :] = here[starts[j] : starts[j] + size]
    for j in chunks:
        some = packed_rows[j]
        value = w_rows[packed_at[j] : packed_at[j] + some, :]
        high = value.astype(bf16).astype(f32)
        pair_rows[:some, :] = high
        pair_rows[some : 2 * some, :] = value - high
        spread[j][...] = pair_rows[: 2 * some, :].T
    x_cols[...] = jnp.zeros(x_cols.shape, bf16)

    with phase("ready"):

        @pl.when(role[1] == 1)
        def _():
            pass_on(0, 0)
            pl.semaphore_wait(ready, quarter)
            dispatch(0, quarter, side)
            pass_on(0, 1)
            for j in chunks[1:]:
                dispatch(j, quarter, side)
                pass_on(j, 0)

    for load in loads[:2]:
        load.wait()
    arrive(0)
    with phase("pass"):

        @pl.when(role[1] == 1)
        def _():
            for j in chunks[1:]:
                pass_on(j, 1)

    last = 1
    lower = 1 - upper
    odd = core

    def when(flag, *steps):
        @pl.when(flag == 1)
        def _():
            for step, *args in steps:
                step(*args)

    def came(j):
        with phase(f"forward{j}"):
            forward(j).wait_recv()

    def send(j):
        swap(j).start()

    when(odd, (to_cols, 2))
    when(odd * lower, (came, 0))
    when(lower, (to_cols, 0))
    when(even, (came, 0), (to_cols, 2))
    loads[2].wait()
    with phase("down0"):
        experts_part(0)
    when(1 - odd * upper, (send, 0))
    arrive(1)
    when(odd, (to_cols, 3))
    when(even, (to_cols, 1))
    when(1 - even * upper, (finish, 0))
    when(odd * upper, (came, 0))
    when(upper, (to_cols, 0))
    came(1)
    when(odd, (to_cols, 1))
    when(even, (to_cols, 3))
    with phase("down1"):
        experts_part(1)
    when(odd * upper, (send, 0))
    send(1)
    when(even * upper, (finish, 0))

    with phase("left"):
        dispatch_left()
        sent(both_chunks(in_x, side * half), f_send)
    finish(last)
    with phase("left"):
        sent(sums.at[pl.ds(0, 2)], q_send)
        returned(0, True)

    for j in chunks:
        if j == last:
            returned(j, True)
        with phase(f"returned{j}"):
            returned(j, False)
        block = 8 * sizes[j]

        def unpack(b):
            got = c_recv[j, block_rows(b, block)].astype(f32)
            flat[: block * pieces, :] = got.reshape(block * pieces, LANES)
            at = packed_at[j] + b * block
            at = at if isinstance(b, int) else pl.multiple_of(at, 8)
            for s in range(pieces):
                r_cols[pl.ds(at, block), s * LANES : (s + 1) * LANES] = flat[
                    pl.ds(s, block, stride=pieces), :
                ]

        loop(experts // 8, unpack)
        here = slice(packed_at[j], packed_at[j] + packed_rows[j])
        for k in range(2):
            part = slice(k * cols, (k + 1) * cols)
            res = r_cols[here, part].astype(bf16)
            twice = jnp.concatenate([res, res], axis=0)
            total = jnp.dot(spread[j][...].astype(bf16), twice, preferred_element_type=f32)
            if j == 0:
                held[:, part] = total
            else:
                mixed[:, part] = (held[:, part] + total).astype(bf16)


def local(n, tokens, norm_gain, chosen_rows, route_weights, gate_weight, up_weight, down_weight):
    tok_rows, width = tokens.shape
    half_rows = tok_rows // 2
    experts, slots = chosen_rows.shape
    half = slots // 2
    sizes = group_sizes(half)
    packed_rows = [round_up(experts * size, 16) for size in sizes]
    parts = len(sizes)
    top = max(sizes)
    side = n // 2
    bunch = min(side, 4)
    blocks = side // bunch
    block = bunch * 2 * top
    pad = round_up(block, 16)
    first_pad = round_up(bunch * 2 * sizes[0], 16)
    pieces = width // LANES
    ff = gate_weight.shape[2]
    bf16, f32 = jnp.bfloat16, jnp.float32
    packed = pltpu.VMEM((parts, n * top, pieces, LANES), bf16)
    vmem = pl.BlockSpec(memory_space=pltpu.VMEM)
    hbm = pl.BlockSpec(memory_space=pltpu.HBM)
    scratch = [
        pltpu.VMEM((tok_rows, width), bf16),
        pltpu.VMEM(norm_gain.shape, norm_gain.dtype),
        pltpu.VMEM(chosen_rows.shape, chosen_rows.dtype),
        pltpu.VMEM(route_weights.shape, route_weights.dtype),
        pltpu.VMEM((width, 2 * ff), bf16),
        pltpu.VMEM(down_weight.shape[1:], bf16),
        packed,
        pltpu.VMEM((4, n * top, pieces, LANES), bf16),
        packed,
        pltpu.VMEM((max(block, 8 * top) * pieces, LANES), f32),
        pltpu.VMEM((blocks, 2 * pad + first_pad, width), bf16),
        pltpu.VMEM((5, blocks, block, width), bf16),
        pltpu.VMEM((2, blocks, block, width), bf16),
        packed,
        packed,
        pltpu.VMEM((n * top, tok_rows), f32),
        pltpu.VMEM((sum(packed_rows), half_rows), f32),
        pltpu.VMEM((2 * max(packed_rows), half_rows), f32),
        pltpu.VMEM((half_rows, 2 * packed_rows[0]), f32),
        pltpu.VMEM((half_rows, 2 * packed_rows[1]), f32),
        pltpu.VMEM((half_rows, width), f32),
        pltpu.VMEM((sum(packed_rows), width), f32),
    ]
    limit = VMEM_BYTES - half_rows * width * 2
    return pl.pallas_call(
        functools.partial(kernel, n),
        out_shape=pltpu.VMEM((half_rows, width), bf16),
        in_specs=[hbm] * 7,
        out_specs=vmem,
        scratch_shapes=scratch
        + [pltpu.SemaphoreType.DMA, pltpu.SemaphoreType.DMA((parts,))] * 3
        + [pltpu.SemaphoreType.DMA((parts,))] * 2
        + [pltpu.SemaphoreType.DMA, pltpu.SemaphoreType.DMA((2 * parts,)), pltpu.SemaphoreType.DMA]
        + [pltpu.SemaphoreType.REGULAR],
        compiler_params=pltpu.CompilerParams(
            collective_id=0, has_side_effects=True, vmem_limit_bytes=limit
        ),
    )(
        tokens,
        norm_gain,
        chosen_rows,
        route_weights,
        gate_weight,
        up_weight,
        down_weight,
    )


def solution(mesh):
    return jax.shard_map(
        functools.partial(local, mesh.shape["ep"]),
        mesh=mesh,
        in_specs=(
            P(("grp", "ep"), None),
            P(),
            P("grp", "ep"),
            P("grp", "ep"),
            P("ep", None, "tp"),
            P("ep", None, "tp"),
            P("ep", "tp", None),
        ),
        out_specs=P(("grp", "ep", "tp"), None),
        check_vma=False,
    )
```
